512 devices in a mesh: ep: 128 (over z, x, core), tp: 4 (over y).
Axes of the slice: x: 4, y: 4, z: 16, core: 2. Of those that a mesh axis runs over, the one named last changes fastest.
Arguments:
- residual: bfloat16 [2048, 1024], P('ep', 'tp'), may hold values from -32 to 32
- cache_keys: bfloat16 [2048, 1024, 256], P(('ep', 'tp')), may hold values from -128 to 128
- cache_values: bfloat16 [2048, 1024, 256], P(('ep', 'tp')), may hold values from -6 to 6
- lengths: int32 [2048], P('ep'), may hold values from 128 to 1024
- query_weight: bfloat16 [1024, 1024], P('tp', 'ep'), may hold values from -0.1875 to 0.1875
- key_weight: bfloat16 [1024, 256], P('tp', 'ep'), may hold values from -0.1875 to 0.1875
- value_weight: bfloat16 [1024, 256], P('tp', 'ep'), may hold values from -0.1875 to 0.1875
- out_weight: bfloat16 [1024, 1024], P('tp', 'ep'), may hold values from -0.1875 to 0.1875
- head_gain: float32 [128], replicated, may hold values from 0.1 to 1.9
- mix_lambda: float32 [8], replicated, may hold values from 0.3 to 0.8
- attn_gain: bfloat16 [1024], P('tp'), may hold values from 0.099609375 to 1.8984375
- moe_gain: bfloat16 [1024], P('tp'), may hold values from 0.099609375 to 1.8984375
- route_ids: int32 [2048, 6], P('ep'), may hold values from 0 to 127, as said below
- route_logits: float32 [2048, 6], P('ep'), may hold values from -8 to 8
- gate_weight: bfloat16 [128, 1024, 512], P('ep', None, 'tp'), may hold values from -0.1875 to 0.1875
- up_weight: bfloat16 [128, 1024, 512], P('ep', None, 'tp'), may hold values from -0.1875 to 0.1875
- down_weight: bfloat16 [128, 512, 1024], P('ep', 'tp'), may hold values from -1.5 to 1.5
Outputs:
- output: bfloat16 [2048, 1024], P('ep', 'tp')
- new_keys: bfloat16 [2048, 256], P('ep')
- new_values: bfloat16 [2048, 256], P('ep')
The draws below stay inside these ranges and needn't reach their ends.
Inputs may be any that keep to these rules, and one draw needn't show every extreme that they name: `route_ids`: the 6 experts of a row are distinct and lie in one group of 8 consecutive experts. Among the 16 rows of one index of ep, no expert is named by more than 2 rows, and some expert is named by exactly 2 of them.
All inputs are finite; a program needn't handle non-finite values.
Results may differ from the reference program's by a relative error of at most 0.013.
The reference program's roundings to bfloat16 on the way count: a program that leaves them out, or rounds other values in their place, can miss the bound.
Values may be sent and summed in bfloat16 or wider, within the bound.
A program may use at most 64 MiB of HBM per device.

```python
import jax
import jax.numpy as jnp
from jax import lax

WIDTH = 1024
HEADS = 8
KV_HEADS = 2
HEAD_DIM = 64
VALUE_DIM = 128
EXPERT_WIDTH = 512
GROUP_SIZE = 8
CHOSEN = 6
SEQ_DEV = 16
CACHE_LEN = 1024
SEQS = 2048
EXPERTS = 128
GROUPS = 16
GROUP_MOST = 2
CAPACITY = 2


def draw_residual(key, part):
    column = jnp.arange(WIDTH, dtype=jnp.float32)
    rising = 0.5 * jnp.exp(jnp.log(4.0) * column / WIDTH)
    drawn = jax.random.truncated_normal(key, -6.0, 6.0, (SEQS, WIDTH), jnp.float32)
    return (drawn * rising[None, :]).astype(jnp.bfloat16)


def draw_cache_keys(key, part):
    array_shape = (SEQS, CACHE_LEN, 2 * KV_HEADS * HEAD_DIM)
    drawn = jax.random.truncated_normal(key, -6.0, 6.0, array_shape, jnp.float32)
    return (1.75 * drawn).astype(jnp.bfloat16)


def route_block(block_key):
    force_key, score_key, token_key, offset_key, label_key = jax.random.split(block_key, 5)
    slot_total = GROUPS * GROUP_MOST
    slot_group = jnp.arange(slot_total, dtype=jnp.int32) // GROUP_MOST
    forced = jax.random.randint(force_key, (), 0, GROUPS)
    scores = jax.random.randint(score_key, (slot_total,), 0, 4096) * slot_total + jnp.arange(slot_total, dtype=jnp.int32)
    scores = jnp.where(slot_group == forced, jnp.arange(slot_total, dtype=jnp.int32) - slot_total, scores)
    picked = jnp.argsort(scores)[:SEQ_DEV]
    picked = picked[jax.random.permutation(token_key, SEQ_DEV)]
    group_id = picked // GROUP_MOST
    slot_rank = picked % GROUP_MOST
    offset = jax.random.randint(offset_key, (GROUPS,), 0, GROUP_SIZE)
    labels = jax.random.permutation(label_key, GROUP_SIZE)
    within = (offset[group_id][:, None] + CHOSEN * slot_rank[:, None] + jnp.arange(CHOSEN)[None, :]) % GROUP_SIZE
    return (group_id[:, None] * GROUP_SIZE + labels[within]).astype(jnp.int32)


def draw_route_ids(key, part):
    blocks = SEQS // SEQ_DEV
    block_keys = jax.random.split(jax.random.fold_in(key, 11), blocks)
    return jax.vmap(route_block)(block_keys).reshape(SEQS, CHOSEN).astype(jnp.int32)


def touch_ends(result, own_key, smallest, high):
    longest = result.shape.index(max(result.shape))
    spots = []
    for shift in (0, 1):
        where = [jax.random.randint(jax.random.fold_in(own_key, axis), (), 0, length) for axis, length in enumerate(result.shape)]
        where[longest] = (where[longest] + shift) % result.shape[longest]
        spots.append(tuple(where))
    return result.at[spots[0]].set(smallest).at[spots[1]].set(high)


def levels(key, shape, cuts, low, top_value):
    level, own = 1.0, jax.random.fold_in(key, 6)
    for position, shards_of in cuts:
        heights = jnp.exp(jax.random.uniform(jax.random.fold_in(own, position), (shards_of,), jnp.float32, low / len(cuts), top_value / len(cuts)))
        level = level * jnp.repeat(heights, shape[position] // shards_of).reshape([-1 if axis == position else 1 for axis in range(len(shape))])
    return level


def gaussian(own_key, shape, deviation, reach, shards=(), held_as=jnp.bfloat16):
    entries = jax.random.normal(own_key, shape, jnp.float32) * deviation
    if len(shards) > 0:
        entries = levels(own_key, shape, shards, -0.22, 0.18) * entries
    return jnp.clip(entries, min=-reach, max=reach).astype(held_as)


def setup_inputs(seed: int = 0) -> dict:
    streams_of = jax.random.split(jax.random.key(seed), 18)
    return {
        "residual": draw_residual(jax.random.fold_in(streams_of[17], 71), 0),
        "cache_keys": draw_cache_keys(jax.random.fold_in(streams_of[17], 71), 0),
        "cache_values": gaussian(streams_of[2], (SEQS, CACHE_LEN, KV_HEADS * VALUE_DIM), 1.0, 6.0, ((0, 512),)),
        "lengths": touch_ends(jax.random.randint(streams_of[3], (SEQS,), CACHE_LEN // 8, CACHE_LEN + 1), jax.random.fold_in(streams_of[3], 1), CACHE_LEN // 8, CACHE_LEN).astype(jnp.int32),
        "query_weight": gaussian(streams_of[4], (WIDTH, 2 * HEADS * HEAD_DIM), WIDTH ** -0.5, 0.1875, ((0, 4), (1, 128))),
        "key_weight": gaussian(streams_of[5], (WIDTH, 2 * KV_HEADS * HEAD_DIM), WIDTH ** -0.5, 0.1875, ((0, 4), (1, 128))),
        "value_weight": gaussian(streams_of[6], (WIDTH, KV_HEADS * VALUE_DIM), WIDTH ** -0.5, 0.1875, ((0, 4), (1, 128))),
        "out_weight": gaussian(streams_of[7], (HEADS * VALUE_DIM, WIDTH), (HEADS * VALUE_DIM) ** -0.5, 0.1875, ((0, 4), (1, 128))),
        "head_gain": jnp.clip(1.0 + 0.18 * jax.random.normal(streams_of[8], (VALUE_DIM,), jnp.float32), 0.1, 1.9),
        "mix_lambda": jnp.clip(jax.random.uniform(streams_of[9], (HEADS,), jnp.float32, 0.3, 0.8), 0.3, 0.8),
        "attn_gain": jnp.clip(1.0 + 0.18 * jax.random.normal(streams_of[10], (WIDTH,), jnp.float32), 0.099609375, 1.8984375).astype(jnp.bfloat16),
        "moe_gain": jnp.clip(1.0 + 0.18 * jax.random.normal(streams_of[11], (WIDTH,), jnp.float32), 0.099609375, 1.8984375).astype(jnp.bfloat16),
        "route_ids": draw_route_ids(jax.random.fold_in(streams_of[17], 71), 0),
        "route_logits": gaussian(streams_of[13], (SEQS, CHOSEN), 2.5, 8.0, ((0, 128),), jnp.float32),
        "gate_weight": gaussian(streams_of[14], (EXPERTS, WIDTH, EXPERT_WIDTH), WIDTH ** -0.5, 0.1875, ((0, 128), (2, 4))),
        "up_weight": gaussian(streams_of[15], (EXPERTS, WIDTH, EXPERT_WIDTH), WIDTH ** -0.5, 0.1875, ((0, 128), (2, 4))),
        "down_weight": gaussian(streams_of[16], (EXPERTS, EXPERT_WIDTH, WIDTH), (EXPERT_WIDTH // 32) ** -0.5, 1.5, ((0, 128), (1, 4))),
    }


norm_eps = 1e-06
head_eps = 1e-05
masked_score = -1e+30
rotary_base = 500000.0

def rotate(blocks, positions):
    half_dim = blocks.shape[-1] // 2
    inverse = rotary_base ** (-jnp.arange(half_dim, dtype=jnp.float32) / half_dim)
    angles = positions[:, None] * inverse[None, :]
    cosine = jnp.cos(angles)[:, None, :]
    sine = jnp.sin(angles)[:, None, :]
    first_half = blocks[..., :half_dim]
    second_half = blocks[..., half_dim:]
    return jnp.concatenate([first_half * cosine - second_half * sine, second_half * cosine + first_half * sine], axis=-1)

def norm_rows(stream, gain, epsilon):
    return stream * lax.rsqrt(lax.optimization_barrier(jnp.mean(stream * stream, axis=-1, keepdims=True)) + epsilon) * gain.astype(jnp.float32)

def reference(residual, cache_keys, cache_values, lengths, query_weight, key_weight, value_weight, out_weight, head_gain, mix_lambda, attn_gain, moe_gain, route_ids, route_logits, gate_weight, up_weight, down_weight):
    seq_total = residual.shape[0]
    groups_per = HEADS // KV_HEADS
    stream = residual.astype(jnp.float32)
    normed = norm_rows(stream, attn_gain, norm_eps).astype(jnp.bfloat16)
    query_raw = jnp.dot(normed, query_weight, preferred_element_type=jnp.float32)
    key_raw = jnp.dot(normed, key_weight, preferred_element_type=jnp.float32)
    new_values = jnp.dot(normed, value_weight, preferred_element_type=jnp.float32).astype(jnp.bfloat16)
    positions = lengths.astype(jnp.float32)
    queries = rotate(query_raw.reshape(seq_total, 2 * HEADS, HEAD_DIM), positions).astype(jnp.bfloat16)
    new_keys = rotate(key_raw.reshape(seq_total, 2 * KV_HEADS, HEAD_DIM), positions).astype(jnp.bfloat16)
    block_count = seq_total // SEQ_DEV
    lambdas = mix_lambda.reshape(KV_HEADS, groups_per)

    def attend_block(operands):
        block_queries, block_keys, block_values, cached_keys, cached_values, block_lengths = operands
        query_heads = block_queries.reshape(SEQ_DEV, KV_HEADS, groups_per, 2, HEAD_DIM).astype(jnp.float32)
        key_heads = block_keys.reshape(SEQ_DEV, KV_HEADS, 2, HEAD_DIM).astype(jnp.float32)
        value_heads = block_values.reshape(SEQ_DEV, KV_HEADS, VALUE_DIM).astype(jnp.float32)
        cache_k = cached_keys.reshape(SEQ_DEV, CACHE_LEN, KV_HEADS, 2, HEAD_DIM).astype(jnp.float32)
        cache_v = cached_values.reshape(SEQ_DEV, CACHE_LEN, KV_HEADS, VALUE_DIM).astype(jnp.float32)
        cache_scores = jnp.einsum('bkgmd,blkmd->bkgml', query_heads, cache_k) / 8.0
        valid = jnp.arange(CACHE_LEN)[None, :] < block_lengths[:, None]
        cache_scores = jnp.where(valid[:, None, None, None, :], cache_scores, masked_score)
        own_scores = jnp.einsum('bkgmd,bkmd->bkgm', query_heads, key_heads) / 8.0
        maxima = jnp.maximum(lax.optimization_barrier(jnp.max(cache_scores, axis=-1)), own_scores)
        cache_weights = jnp.exp(cache_scores - maxima[..., None]).astype(jnp.bfloat16).astype(jnp.float32)
        own_weights = jnp.exp(own_scores - maxima).astype(jnp.bfloat16).astype(jnp.float32)
        denominator = lax.optimization_barrier(jnp.sum(cache_weights, axis=-1)) + own_weights
        weighted = jnp.einsum('bkgml,blkv->bkgmv', cache_weights, cache_v) + own_weights[..., None] * value_heads[:, :, None, None, :]
        averaged = weighted / denominator[..., None]
        contrast = averaged[:, :, :, 0] - lambdas[None, :, :, None] * averaged[:, :, :, 1]
        contrast = norm_rows(contrast, head_gain, head_eps)
        return contrast.astype(jnp.bfloat16).reshape(SEQ_DEV, HEADS * VALUE_DIM)
    heads_out = lax.map(attend_block, (queries.reshape(block_count, SEQ_DEV, -1), new_keys.reshape(block_count, SEQ_DEV, -1), new_values.reshape(block_count, SEQ_DEV, -1), cache_keys.reshape(block_count, SEQ_DEV, CACHE_LEN, -1), cache_values.reshape(block_count, SEQ_DEV, CACHE_LEN, -1), lengths.reshape(block_count, SEQ_DEV))).reshape(seq_total, HEADS * VALUE_DIM)
    attended = jnp.dot(heads_out, out_weight, preferred_element_type=jnp.float32)
    middle = (stream + attended).astype(jnp.bfloat16)
    middle_wide = middle.astype(jnp.float32)
    mixed_in = norm_rows(middle_wide, moe_gain, norm_eps).astype(jnp.bfloat16)
    expert_count = gate_weight.shape[0]
    block_ids = route_ids.reshape(block_count, SEQ_DEV * CHOSEN).astype(jnp.int32)

    def ranks_of(one_block):
        matches = one_block[:, None] == one_block[None, :]
        earlier = jnp.arange(one_block.shape[0])[:, None] > jnp.arange(one_block.shape[0])[None, :]
        return lax.optimization_barrier(jnp.sum(jnp.logical_and(matches, earlier), axis=1)).astype(jnp.int32)
    slot_rank = jax.vmap(ranks_of)(block_ids)
    rows_in_expert = (jnp.arange(block_count, dtype=jnp.int32)[:, None] * CAPACITY + slot_rank).astype(jnp.int32)
    buffer_index = (block_ids * (block_count * CAPACITY) + rows_in_expert).reshape(-1).astype(jnp.int32)
    token_index = (jnp.arange(seq_total * CHOSEN, dtype=jnp.int32) // CHOSEN).astype(jnp.int32)
    buffers = jnp.zeros((expert_count * block_count * CAPACITY, WIDTH), jnp.bfloat16).at[buffer_index].set(mixed_in[token_index])

    def run_expert(operands):
        slot_rows, gate_mat, up_mat, down_mat = operands
        gate_act = jnp.dot(slot_rows, gate_mat, preferred_element_type=jnp.float32)
        up_act = jnp.dot(slot_rows, up_mat, preferred_element_type=jnp.float32)
        hidden = (jax.nn.silu(gate_act) * up_act).astype(jnp.bfloat16)
        return jnp.dot(hidden, down_mat, preferred_element_type=jnp.float32).astype(jnp.bfloat16)
    produced = lax.map(run_expert, (buffers.reshape(expert_count, block_count * CAPACITY, WIDTH), gate_weight, up_weight, down_weight))
    picked = produced.reshape(-1, WIDTH)[buffer_index].reshape(seq_total, CHOSEN, WIDTH)
    gates = jax.nn.softmax(route_logits.astype(jnp.float32), axis=-1)
    output = (middle_wide + lax.optimization_barrier(jnp.sum(gates[..., None] * picked.astype(jnp.float32), axis=1))).astype(jnp.bfloat16)
    return (output, new_keys.reshape(seq_total, -1), new_values)
```

```python
import jax
import jax.numpy as jnp
from jax import lax
from jax.experimental import pallas as pl
from jax.experimental.pallas import tpu as pltpu
from jax.sharding import Mesh
from jax.sharding import PartitionSpec as P

WIDTH = 1024
HEADS = 8
HEAD_DIM = 64
VALUE_DIM = 128
CHOSEN = 6
GROUP_SIZE = 8
SLOTS = 2
EP = ("ep_0", "ep_1", "ep_2")
EP_TP = ("ep_0", "ep_1", "ep_2", "tp")
NZ, NX, NC, NY = 16, 4, 2, 4
NG = NX * NC
NP = NG * NY
CACHE = 1024
OWN = 4

norm_eps = 1e-06
head_eps = 1e-05
masked_score = -1e30
rotary_base = 500000.0

MESH = pl.DeviceIdType.MESH
BF = jnp.bfloat16
F32 = jnp.float32


def nt(a, b):
    return lax.dot_general(a, b, (((1,), (1,)), ((), ())), preferred_element_type=F32)


def nn(a, b):
    return lax.dot_general(a, b, (((1,), (0,)), ((), ())), preferred_element_type=F32)


def far_first(k, n):
    half = lax.div(k + 1, 2)
    return jnp.where(lax.rem(k, 2) == 1, n // 2 + half, n // 2 - half)


def iota(shape, dim):
    return lax.broadcasted_iota(jnp.int32, shape, dim)


def kernel(
    res_ref,
    ck_hbm,
    cv_hbm,
    lens_ref,
    wq_ref,
    wk_ref,
    wv_ref,
    wo_ref,
    hgain_ref,
    lam_ref,
    again_ref,
    mgain_ref,
    rid_ref,
    ridt_ref,
    logits_ref,
    gate_hbm,
    up_hbm,
    down_hbm,
    cos_ref,
    sin_ref,
    out_ref,
    nk_ref,
    nv_ref,
    kbuf,
    vbuf,
    gbuf,
    ubuf,
    dbuf,
    loc_sem,
    wqkv,
    wz,
    wos,
    woz,
    woa,
    sqs,
    sqr,
    nall,
    mgs,
    mga,
    sb,
    rb,
    ebuf,
    kvs,
    kvr,
    kvo,
    hb,
    hr,
    lhs,
    ob,
    orr,
    gz_s,
    gz_r,
    gown,
    gall,
    ds,
    dr,
    xb,
    cs,
    cr,
    fs,
    fr,
    zs,
    zr,
    s_wz,
    r_wz,
    s_wo,
    r_wo,
    s_woa,
    r_woa,
    s_sq,
    r_sq,
    s_na,
    r_na,
    s_mg,
    r_mg,
    s_rb,
    r_rb,
    s_kv,
    r_kv,
    s_h,
    r_h,
    s_o,
    r_o,
    s_gz,
    r_gz,
    s_ga,
    r_ga,
    s_d,
    r_d,
    s_x,
    r_x,
    s_xc,
    r_xc,
    s_cs,
    r_cs,
    s_f,
    r_f,
    s_z,
    r_z,
):
    z = lax.axis_index("ep_0")
    x = lax.axis_index("ep_1")
    c = lax.axis_index("ep_2")
    y = lax.axis_index("tp")
    g = x * NC + c
    p = g * NY + y
    q16 = x * NY + y

    def plane_id(other):
        og = lax.div(other, NY)
        return {"ep_1": lax.div(og, NC), "ep_2": lax.rem(og, NC), "tp": lax.rem(other, NY)}

    def to(src, dst, ssem, rsem, dev):
        pltpu.make_async_remote_copy(
            src_ref=src, dst_ref=dst, send_sem=ssem, recv_sem=rsem, device_id=dev, device_id_type=MESH
        ).start()

    def drain(ref, sem):
        pltpu.make_async_copy(ref, ref, sem).wait()

    local = [
        pltpu.make_async_copy(ck_hbm, kbuf, loc_sem.at[0]),
        pltpu.make_async_copy(cv_hbm, vbuf, loc_sem.at[1]),
        pltpu.make_async_copy(gate_hbm, gbuf, loc_sem.at[2]),
        pltpu.make_async_copy(up_hbm, ubuf, loc_sem.at[3]),
        pltpu.make_async_copy(down_hbm, dbuf, loc_sem.at[4]),
    ]
    for copy in local:
        copy.start()

    barrier = pltpu.get_barrier_semaphore()

    @pl.loop(0, NZ - 1)
    def _(k):
        pl.semaphore_signal(
            barrier, inc=1, device_id={"ep_0": lax.rem(z + far_first(k, NZ), NZ)}, device_id_type=MESH
        )

    @pl.loop(1, NP)
    def _(k):
        pl.semaphore_signal(
            barrier, inc=1, device_id=plane_id(lax.rem(p + k, NP)), device_id_type=MESH
        )

    wqkv[...] = jnp.concatenate(
        [
            wq_ref[...].astype(F32),
            wk_ref[...].astype(F32),
            wv_ref[...].astype(F32),
            jnp.zeros((4, 256), F32),
        ],
        axis=0,
    ).astype(BF)
    wz[z] = wqkv[...]
    wos[...] = wo_ref[...]
    woz[z] = wo_ref[...]
    stream = res_ref[...].astype(F32)
    own_squares = jnp.broadcast_to(jnp.sum(stream * stream, axis=1, keepdims=True), (16, 128))
    sqs[...] = own_squares
    mgs[...] = jnp.broadcast_to(mgain_ref[...].astype(F32), (8, 256))

    gcol = lax.shift_right_logical(rid_ref[:, 0:1], 3)
    grow = lax.shift_right_logical(ridt_ref[0:1, :], 3)
    same = (gcol == grow).astype(jnp.int32)
    earlier_col = (iota((16, 16), 1) < iota((16, 16), 0)).astype(jnp.int32)
    earlier_row = (iota((16, 16), 0) < iota((16, 16), 1)).astype(jnp.int32)
    rank_col = jnp.sum((same * earlier_col).astype(F32), axis=1, keepdims=True).astype(jnp.int32)
    rank_row = jnp.sum((same * earlier_row).astype(F32), axis=0, keepdims=True).astype(jnp.int32)
    dispatch = (iota((32, 16), 0) == grow * SLOTS + rank_row).astype(F32)
    combine = (iota((16, 32), 1) == gcol * SLOTS + rank_col).astype(F32)
    logits = logits_ref[...]
    exps = jnp.exp(logits - jnp.max(logits, axis=1, keepdims=True))
    gates = exps / jnp.sum(exps, axis=1, keepdims=True)
    members = jnp.zeros((16, 128), F32)
    for k in range(CHOSEN):
        member = jnp.bitwise_and(rid_ref[:, k : k + 1], GROUP_SIZE - 1)
        members = members + jnp.where(iota((16, 128), 1) == member, gates[:, k : k + 1], 0.0)
    slot_gates = lax.dot_general(
        dispatch, members, (((1,), (0,)), ((), ())), precision=lax.Precision.HIGHEST,
        preferred_element_type=F32,
    )
    for k in range(NZ):
        gz_s[k] = slot_gates[2 * k : 2 * k + 2]
    gz_r[z] = gz_s[z]

    row = iota((1024, 256), 0)
    col = iota((1024, 256), 1)
    src_g = lax.shift_right_logical(row, 7)
    src_z = jnp.bitwise_and(lax.shift_right_logical(row, 4), 7)
    src_r = jnp.bitwise_and(row, 15)
    to_query = jnp.logical_and(src_r < 8, jnp.bitwise_and(col, 63) == src_g * 8 + src_r)
    ebuf[:, 0:256] = jnp.where(to_query, 1.0, 0.0).astype(BF)
    spot = src_z * 16 + src_g * 2
    to_key = jnp.logical_and(
        jnp.logical_and(src_r >= 8, src_r < 10), col == spot + src_r - 8
    )
    to_value = jnp.logical_and(
        jnp.logical_and(src_r >= 10, src_r < 12), col == 128 + spot + src_r - 10
    )
    ebuf[:, 256:512] = jnp.where(jnp.logical_or(to_key, to_value), 1.0, 0.0).astype(BF)

    pl.semaphore_wait(barrier, NZ - 1 + NP - 1)

    @pl.loop(1, NY)
    def _(k):
        dev = {"tp": lax.rem(y + k, NY)}
        to(sqs, sqr.at[y], s_sq, r_sq, dev)
        to(mgs, mga.at[y], s_mg, r_mg, dev)

    @pl.loop(0, NZ - 1)
    def _(k):
        to(wqkv, wz.at[z], s_wz, r_wz, {"ep_0": lax.rem(z + far_first(k, NZ), NZ)})

    @pl.loop(0, NZ - 1)
    def _(k):
        dest = lax.rem(z + far_first(k, NZ), NZ)
        to(wos, woz.at[z], s_wo, r_wo, {"ep_0": dest})
        to(gz_s.at[dest], gz_r.at[z], s_gz, r_gz, {"ep_0": dest})

    sqr[y] = own_squares
    mga[y] = mgs[...]
    drain(sqr.at[pl.ds(0, NY - 1)], r_sq)
    squares = sqr[0] + sqr[1] + sqr[2] + sqr[3]
    scale = lax.rsqrt(squares[:, 0:1] / WIDTH + norm_eps)
    normed = (stream * scale * again_ref[...].astype(F32)).astype(BF)
    nall[g] = normed

    @pl.loop(1, NG)
    def _(k):
        other = lax.rem(g + k, NG)
        to(
            nall.at[g], nall.at[g], s_na, r_na,
            {"ep_1": lax.div(other, NC), "ep_2": lax.rem(other, NC)},
        )

    drain(nall.at[pl.ds(0, NG - 1)], r_na)
    drain(wz.at[pl.ds(0, NZ - 1)], r_wz)
    partial = nt(nall[...].reshape(128, 256), wz[...].reshape(256, 256))
    for k in range(NP):
        sb[k, 0:4, :] = partial[4 * k : 4 * k + 4, 0:128]
        sb[k, 4:8, :] = partial[4 * k : 4 * k + 4, 128:256]

    @pl.loop(1, NP)
    def _(k):
        other = lax.rem(p + k, NP)
        to(sb.at[other], rb.at[p], s_rb, r_rb, plane_id(other))

    rb[p] = sb[p]

    drain(woz.at[pl.ds(0, NZ - 1)], r_wo)
    drain(gz_r.at[pl.ds(0, NZ - 1)], r_gz)
    for k in range(NZ):
        gown[2 * k : 2 * k + 2, :] = gz_r[k]
    gall[g] = gown[...]
    woa[:, g] = woz[...]

    @pl.loop(1, NG)
    def _(k):
        other = lax.rem(g + k, NG)
        dev = {"ep_1": lax.div(other, NC), "ep_2": lax.rem(other, NC)}
        to(woz, woa.at[:, g], s_woa, r_woa, dev)
        to(gown, gall.at[g], s_ga, r_ga, dev)

    drain(rb.at[pl.ds(0, NP - 1)], r_rb)
    parts = rb[...].reshape(NG, NY, 8, 128)
    raw = parts[:, 0] + parts[:, 1] + parts[:, 2] + parts[:, 3]
    lane = iota((8, 128), 1)
    r_of = jnp.bitwise_and(lane, 15)
    is_query = r_of < 8
    is_key = jnp.logical_and(r_of >= 8, r_of < 10)
    low_key = jnp.bitwise_and(lane, 63) < 32
    turned = []
    for k in range(NG):
        own = raw[k]
        pair = raw[(k + NG // 2) % NG]
        if k < NG // 2:
            pair = -pair
        above = pltpu.roll(own, 96, 1)
        below = pltpu.roll(own, 32, 1)
        key_pair = jnp.where(low_key, -above, below)
        spun = own * cos_ref[k] + jnp.where(is_query, pair, key_pair) * sin_ref[k]
        turned.append(jnp.where(jnp.logical_or(is_query, is_key), spun, own))
    rows8 = jnp.concatenate([t.astype(BF) for t in turned], axis=1)
    placed = nn(rows8, ebuf[:, 256:512])
    kvs[...] = placed
    kvr[y] = placed

    @pl.loop(1, NY)
    def _(k):
        to(kvs, kvr.at[y], s_kv, r_kv, {"tp": lax.rem(y + k, NY)})

    own_keys = jnp.concatenate([placed[0:4, 0:128], placed[4:8, 0:128]], axis=1)
    own_values = jnp.concatenate([placed[0:4, 128:256], placed[4:8, 128:256]], axis=1)

    sub = iota((8, 128), 0)
    pieces = []
    for s in range(OWN):
        for m in range(2):
            keep = jnp.logical_and(
                is_query,
                lax.shift_right_logical(lane, 4) == jnp.bitwise_and(2 * sub + m, 7),
            )
            line = []
            for k in range(NG):
                low = jnp.broadcast_to(turned[k][s : s + 1, :], (8, 128))
                high = jnp.broadcast_to(turned[k][4 + s : 5 + s, :], (8, 128))
                line.append(jnp.where(keep, jnp.where(sub < 4, low, high), 0.0))
            pieces.append(jnp.concatenate(line, axis=1))
    spread = nn(jnp.concatenate(pieces, axis=0).astype(BF), ebuf[:, 0:256])
    for copy in local:
        copy.wait()
    blk = lax.shift_right_logical(iota((16, 256), 1), 6)
    row16 = iota((16, 256), 0)
    own_block = (
        lax.shift_right_logical(jnp.bitwise_and(row16, 7), 2) * 2 + lax.shift_right_logical(row16, 3)
    )
    head_low = jnp.bitwise_and(iota((16, 128), 0), 7) < 4
    lam = lam_ref[...]
    for s in range(OWN):
        queries = jnp.where(blk == own_block, spread[16 * s : 16 * s + 16], 0.0)
        scores = nt(queries.astype(BF), kbuf[s]) * 0.125
        length = lens_ref[y * OWN + s]
        scores = jnp.where(iota((16, CACHE), 1) < length, scores, masked_score)
        fresh = jnp.sum(queries * own_keys[s : s + 1], axis=1, keepdims=True) * 0.125
        top = jnp.maximum(jnp.max(scores, axis=1, keepdims=True), fresh)
        weights = jnp.exp(scores - top).astype(BF)
        fresh_weight = jnp.exp(fresh - top).astype(BF).astype(F32)
        total = jnp.sum(weights.astype(F32), axis=1, keepdims=True) + fresh_weight
        mixed = nn(weights, vbuf[s])
        values = jnp.where(
            head_low,
            mixed[:, 0:128] + fresh_weight * own_values[s : s + 1, 0:128],
            mixed[:, 128:256] + fresh_weight * own_values[s : s + 1, 128:256],
        )
        averaged = values / total
        contrast = averaged[0:8] - lam * averaged[8:16]
        contrast = (
            contrast
            * lax.rsqrt(jnp.mean(contrast * contrast, axis=1, keepdims=True) + head_eps)
            * hgain_ref[...]
        )
        rounded = contrast.astype(BF).astype(F32)
        for h in range(HEADS):
            hb[h // 2, h % 2, s : s + 1, :] = rounded[h : h + 1, :]

    hr[y] = hb[y]

    @pl.loop(1, NY)
    def _(k):
        other = lax.rem(y + k, NY)
        to(hb.at[other], hr.at[y], s_h, r_h, {"tp": other})

    drain(woa.at[:, pl.ds(0, NG - 1)], r_woa)
    drain(hr.at[pl.ds(0, NY - 1)], r_h)
    for k in range(NY):
        lhs[4 * k : 4 * k + 4, 0:128] = hr[k, 0]
        lhs[4 * k : 4 * k + 4, 128:256] = hr[k, 1]
    projected = nt(lhs[0:16].astype(BF), woa[...].reshape(WIDTH, 256))
    for k in range(NY):
        ob[k] = projected[:, 256 * k : 256 * k + 256]

    @pl.loop(1, NY)
    def _(k):
        other = lax.rem(y + k, NY)
        to(ob.at[other], orr.at[y], s_o, r_o, {"tp": other})

    orr[y] = ob[y]
    drain(orr.at[pl.ds(0, NY - 1)], r_o)
    attended = orr[0] + orr[1] + orr[2] + orr[3]
    middle = (stream + attended).astype(BF)

    routed = nn(dispatch.astype(BF), middle)
    for k in range(NZ):
        ds[k] = routed[2 * k : 2 * k + 2].astype(ds.dtype)
    dr[z] = ds[z]

    @pl.loop(0, NZ - 1)
    def _(k):
        dest = lax.rem(z + far_first(k, NZ), NZ)
        to(ds.at[dest], dr.at[z], s_d, r_d, {"ep_0": dest})

    drain(dr.at[pl.ds(0, NZ - 1)], r_d)
    for k in range(NZ):
        lhs[2 * k : 2 * k + 2, :] = dr[k].astype(F32)
    xb[x, c, y] = lhs[...].astype(BF)

    @pl.loop(1, NX * NY)
    def _(k):
        other = lax.rem(q16 + k, NX * NY)
        to(
            xb.at[x, c, y], xb.at[x, c, y], s_x, r_x.at[k],
            {"ep_1": lax.div(other, NY), "tp": lax.rem(other, NY)},
        )

    partner = {"ep_2": 1 - c}
    to(xb.at[x, c, y], xb.at[x, c, y], s_xc, r_xc, partner)

    @pl.loop(1, NX * NY)
    def _(k):
        other = lax.rem(q16 + NX * NY - k, NX * NY)
        ox, oy = lax.div(other, NY), lax.rem(other, NY)
        drain(xb.at[ox, c, oy], r_x.at[k])
        to(xb.at[ox, c, oy], xb.at[ox, c, oy], s_xc, r_xc, partner)

    drain(xb.at[:, 0], r_xc)
    drain(gall.at[pl.ds(0, NG - 1)], r_ga)
    drain(mga.at[pl.ds(0, NY - 1)], r_mg)

    wide = [xb[:, :, k].reshape(256, 256).astype(F32) for k in range(NY)]
    total_sq = jnp.zeros((256, 1), F32)
    for k in range(NY):
        total_sq = total_sq + jnp.sum(wide[k] * wide[k], axis=1, keepdims=True)
    scale = lax.rsqrt(total_sq / WIDTH + norm_eps)
    gate_act = jnp.zeros((256, 128), F32)
    up_act = jnp.zeros((256, 128), F32)
    for k in range(NY):
        mixed_in = (wide[k] * scale * mga[k, 0:1, :]).astype(BF)
        gate_act = gate_act + nn(mixed_in, gbuf[0, 256 * k : 256 * k + 256, :])
        up_act = up_act + nn(mixed_in, ubuf[0, 256 * k : 256 * k + 256, :])
    hidden = (gate_act / (1.0 + jnp.exp(-gate_act)) * up_act).astype(BF)
    slot_gate = jnp.sum(
        jnp.where(iota((256, 128), 1) == g, gall[...].reshape(256, 128), 0.0), axis=1, keepdims=True
    )
    produced = (nn(hidden, dbuf[0]) * slot_gate).reshape(NX, NC, 32, WIDTH)

    for k in range(NX):
        mine = jnp.where(c == 0, produced[k, 0], produced[k, 1])
        theirs = jnp.where(c == 0, produced[k, 1], produced[k, 0])
        for j in range(NY):
            cs[k, j] = theirs[:, 256 * j : 256 * j + 256].astype(BF)
            fs[k, j] = mine[:, 256 * j : 256 * j + 256]
    to(cs, cr, s_cs, r_cs, partner)
    drain(cr, r_cs)
    both = fs[...] + cr[...].astype(F32)
    fb = cs
    drain(cs, s_cs)
    fb[...] = both.astype(BF)

    @pl.loop(1, NX * NY)
    def _(k):
        other = lax.rem(q16 + k, NX * NY)
        ox, oy = lax.div(other, NY), lax.rem(other, NY)
        to(fb.at[ox, oy], fr.at[q16], s_f, r_f, {"ep_1": ox, "tp": oy})

    fr[q16] = fb[x, y]
    drain(fr.at[pl.ds(0, NX * NY - 1)], r_f)
    mixture = fr[0].astype(F32)
    for k in range(1, NX * NY):
        mixture = mixture + fr[k].astype(F32)
    for k in range(NZ):
        zs[k] = mixture[2 * k : 2 * k + 2].astype(zs.dtype)
    zr[z] = zs[z]

    @pl.loop(0, NZ - 1)
    def _(k):
        dest = lax.rem(z + far_first(k, NZ), NZ)
        to(zs.at[dest], zr.at[z], s_z, r_z, {"ep_0": dest})

    drain(kvr.at[pl.ds(0, NY - 1)], r_kv)
    for k in range(NY):
        for half in range(2):
            kvo[4 * k : 4 * k + 4, 128 * half : 128 * half + 128] = kvr[k, 4 * half : 4 * half + 4, 0:128]
            kvo[4 * k : 4 * k + 4, 256 + 128 * half : 384 + 128 * half] = kvr[
                k, 4 * half : 4 * half + 4, 128:256
            ]
    nk_ref[...] = kvo[:, 0:256].astype(BF)
    nv_ref[...] = kvo[:, 256:512].astype(BF)

    drain(zr.at[pl.ds(0, NZ - 1)], r_z)
    for k in range(NZ):
        lhs[2 * k : 2 * k + 2, :] = zr[k].astype(F32)
    mix = nn(combine.astype(BF), lhs[...].astype(BF))
    out_ref[...] = (middle.astype(F32) + mix).astype(BF)

    for ref, sem in (
        (wz, s_wz),
        (woz, s_wo),
        (gz_r, s_gz),
        (dr, s_d),
        (zr, s_z),
    ):
        drain(ref.at[pl.ds(0, NZ - 1)], sem)
    for ref, sem in ((sqr, s_sq), (mga, s_mg), (kvr, s_kv), (hr, s_h), (orr, s_o)):
        drain(ref.at[pl.ds(0, NY - 1)], sem)
    for ref, sem in ((nall, s_na), (gall, s_ga)):
        drain(ref.at[pl.ds(0, NG - 1)], sem)
    drain(woa.at[:, pl.ds(0, NG - 1)], s_woa)
    drain(rb.at[pl.ds(0, NP - 1)], s_rb)
    drain(fr.at[pl.ds(0, NX * NY - 1)], s_x)
    drain(fr.at[pl.ds(0, NX * NY - 1)], s_f)
    drain(xb.at[:, 0], s_xc)


def on_device(
    residual,
    cache_keys,
    cache_values,
    lengths,
    query_weight,
    key_weight,
    value_weight,
    out_weight,
    head_gain,
    mix_lambda,
    attn_gain,
    moe_gain,
    route_ids,
    route_logits,
    gate_weight,
    up_weight,
    down_weight,
):
    y = lax.axis_index("tp")
    half_dim = HEAD_DIM // 2
    inverse = rotary_base ** (-jnp.arange(half_dim, dtype=F32) / half_dim)
    gg = jnp.arange(NG)[:, None]
    lane = jnp.arange(128)[None, :]
    r_of = lane % 16
    at_query = (gg % (NG // 2)) * 8 + r_of % 8
    at_key = ((lane // 16) % 2) * 16 + gg * 2 + r_of % 2
    entry = jnp.where(r_of < 8, at_query, at_key)
    table = inverse[entry]
    own = lax.dynamic_slice_in_dim(lengths, y * OWN, OWN, 0).astype(F32)
    rows = jnp.concatenate([own, own])
    angles = rows[None, :, None] * table[:, None, :]
    cosine, sine = jnp.cos(angles), jnp.sin(angles)

    vm = pl.BlockSpec(memory_space=pltpu.VMEM)
    hbm = pl.BlockSpec(memory_space=pl.ANY)
    smem = pl.BlockSpec(memory_space=pltpu.SMEM)
    dma = pltpu.SemaphoreType.DMA
    V = pltpu.VMEM
    scratch = [
        V((OWN, CACHE, 256), BF),
        V((OWN, CACHE, 256), BF),
        V((1, WIDTH, 128), BF),
        V((1, WIDTH, 128), BF),
        V((1, 128, WIDTH), BF),
        dma((5,)),
        V((16, 256), BF),
        V((NZ, 16, 256), BF),
        V((8, 256), BF),
        V((NZ, 8, 256), BF),
        V((NZ, NG, 8, 256), BF),
        V((16, 128), F32),
        V((NY, 16, 128), F32),
        V((NG, 16, 256), BF),
        V((8, 256), F32),
        V((NY, 8, 256), F32),
        V((NP, 8, 128), F32),
        V((NP, 8, 128), F32),
        V((1024, 512), BF),
        V((8, 256), F32),
        V((NY, 8, 256), F32),
        V((16, 512), F32),
        V((NY, 2, OWN, 128), F32),
        V((NY, 2, OWN, 128), F32),
        V((32, 256), F32),
        V((NY, 16, 256), F32),
        V((NY, 16, 256), F32),
        V((NZ, SLOTS, 128), F32),
        V((NZ, SLOTS, 128), F32),
        V((32, 128), F32),
        V((NG, 32, 128), F32),
        V((NZ, SLOTS, 256), F32),
        V((NZ, SLOTS, 256), F32),
        V((NX, NC, NY, 32, 256), BF),
        V((NX, NY, 32, 256), BF),
        V((NX, NY, 32, 256), BF),
        V((NX, NY, 32, 256), F32),
        V((NX * NY, 32, 256), BF),
        V((NZ, SLOTS, 256), F32),
        V((NZ, SLOTS, 256), F32),
    ]
    sems = [dma] * 36
    sems[27] = dma((NX * NY,))
    out, nk, nv = pl.pallas_call(
        kernel,
        out_shape=(
            jax.ShapeDtypeStruct((16, 256), BF),
            jax.ShapeDtypeStruct((16, 256), BF),
            jax.ShapeDtypeStruct((16, 256), BF),
        ),
        in_specs=[vm, hbm, hbm, smem] + [vm] * 11 + [hbm] * 3 + [vm] * 2,
        out_specs=(vm, vm, vm),
        scratch_shapes=scratch + sems,
        compiler_params=pltpu.CompilerParams(
            collective_id=0, has_side_effects=True, vmem_limit_bytes=40 * 2**20
        ),
        cost_estimate=pl.CostEstimate(flops=10**9, bytes_accessed=5 * 10**6, transcendentals=0),
    )(
        residual,
        cache_keys,
        cache_values,
        lengths,
        query_weight.T,
        key_weight.T,
        value_weight.T,
        out_weight.T,
        head_gain.reshape(1, 128),
        mix_lambda.reshape(HEADS, 1),
        attn_gain.reshape(1, 256),
        moe_gain.reshape(1, 256),
        route_ids,
        route_ids.T,
        route_logits,
        gate_weight,
        up_weight,
        down_weight,
        cosine,
        sine,
    )
    return out, nk, nv


def solution(mesh):
    torus = Mesh(mesh.devices.reshape(NZ, NX, NC, NY), ("ep_0", "ep_1", "ep_2", "tp"))
    return jax.shard_map(
        on_device,
        mesh=torus,
        in_specs=(
            P(EP, "tp"),
            P(EP_TP, None, None),
            P(EP_TP, None, None),
            P(EP),
            P("tp", EP),
            P("tp", EP),
            P("tp", EP),
            P("tp", EP),
            P(),
            P(),
            P("tp"),
            P("tp"),
            P(EP, None),
            P(EP, None),
            P(EP, None, "tp"),
            P(EP, None, "tp"),
            P(EP, "tp", None),
        ),
        out_specs=(P(EP, "tp"), P(EP, None), P(EP, None)),
        check_vma=False,
    )
```

```python
import math

import jax
import jax.numpy as jnp
from jax import lax
from jax.experimental import pallas as pl
from jax.experimental.pallas import tpu as pltpu
from jax.sharding import Mesh
from jax.sharding import PartitionSpec as P

WIDTH = 1024
HEADS = 8
HEAD_DIM = 64
VALUE_DIM = 128
CHOSEN = 6
GROUP_SIZE = 8
SLOTS = 2
EP = ("ep_0", "ep_1", "ep_2")
EP_TP = ("ep_0", "ep_1", "ep_2", "tp")
NZ, NX, NC, NY = 16, 4, 2, 4
NG = NX * NC
NP = NG * NY
CACHE = 1024
OWN = 4

norm_eps = 1e-06
head_eps = 1e-05
masked_score = -1e30
rotary_base = 500000.0

MESH = pl.DeviceIdType.MESH
BF = jnp.bfloat16
F32 = jnp.float32


def nt(a, b):
    return lax.dot_general(a, b, (((1,), (1,)), ((), ())), preferred_element_type=F32)


def nn(a, b):
    return lax.dot_general(a, b, (((1,), (0,)), ((), ())), preferred_element_type=F32)


def far_first(k, n):
    half = lax.div(k + 1, 2)
    return jnp.where(lax.rem(k, 2) == 1, n // 2 + half, n // 2 - half)


def iota(shape, dim):
    return lax.broadcasted_iota(jnp.int32, shape, dim)


def kernel(
    res_hbm,
    ck_hbm,
    cv_hbm,
    lens_hbm,
    wq_hbm,
    wk_hbm,
    wv_hbm,
    wo_hbm,
    hgain_hbm,
    lam_hbm,
    again_hbm,
    mgain_hbm,
    ridt_hbm,
    logitst_hbm,
    gate_hbm,
    up_hbm,
    down_hbm,
    out_ref,
    res_ref,
    lens_ref,
    wq_ref,
    wk_ref,
    wv_ref,
    wo_ref,
    hgain_ref,
    lam_ref,
    again_ref,
    mgain_ref,
    ridt_ref,
    logitst_ref,
    kbuf,
    vbuf,
    gbuf,
    ubuf,
    dbuf,
    loc_sem,
    wqkv,
    wz,
    wos,
    woz,
    woa,
    sqs,
    sqr,
    nall,
    mgs,
    mga,
    sb,
    rb,
    ebuf,
    cosb,
    sinb,
    kvs,
    kvr,
    kvo,
    hb,
    hr,
    lhs,
    ob,
    orr,
    gz_s,
    gz_r,
    gown,
    gall,
    ds,
    dr,
    xb,
    fs,
    fr,
    zs,
    zr,
    s_wz,
    r_wz,
    s_wo,
    r_wo,
    s_woa,
    r_woa,
    s_sq,
    r_sq,
    s_na,
    r_na,
    s_mg,
    r_mg,
    s_rb,
    r_rb,
    s_kv,
    r_kv,
    s_h,
    r_h,
    s_o,
    r_o,
    s_gz,
    r_gz,
    s_ga,
    r_ga,
    s_d,
    r_d,
    s_x,
    r_x,
    s_ew,
    r_ew,
    s_f,
    r_f,
    s_z,
    r_z,
):
    z = lax.axis_index("ep_0")
    x = lax.axis_index("ep_1")
    c = lax.axis_index("ep_2")
    y = lax.axis_index("tp")
    g = x * NC + c
    p = g * NY + y
    q16 = x * NY + y

    def plane_id(other):
        og = lax.div(other, NY)
        return {"ep_1": lax.div(og, NC), "ep_2": lax.rem(og, NC), "tp": lax.rem(other, NY)}

    def to(src, dst, ssem, rsem, dev):
        pltpu.make_async_remote_copy(
            src_ref=src, dst_ref=dst, send_sem=ssem, recv_sem=rsem, device_id=dev, device_id_type=MESH
        ).start()

    def drain(ref, sem):
        pltpu.make_async_copy(ref, ref, sem).wait()

    barrier = pltpu.get_barrier_semaphore()

    @pl.loop(0, NZ - 1)
    def _(k):
        pl.semaphore_signal(
            barrier, inc=1, device_id={"ep_0": lax.rem(z + far_first(k, NZ), NZ)}, device_id_type=MESH
        )

    @pl.loop(1, NP)
    def _(k):
        pl.semaphore_signal(
            barrier, inc=1, device_id=plane_id(lax.rem(p + k, NP)), device_id_type=MESH
        )

    small = [
        pltpu.make_async_copy(src, dst, loc_sem.at[k])
        for k, (src, dst) in enumerate(
            (
                (res_hbm, res_ref),
                (wq_hbm, wq_ref),
                (wk_hbm, wk_ref),
                (wv_hbm, wv_ref),
                (wo_hbm, wo_ref),
                (mgain_hbm, mgain_ref),
                (again_hbm, again_ref),
                (hgain_hbm, hgain_ref),
                (ridt_hbm, ridt_ref),
                (logitst_hbm, logitst_ref),
                (lens_hbm, lens_ref),
                (lam_hbm, lam_ref),
            )
        )
    ]
    experts = [
        pltpu.make_async_copy(gate_hbm.at[0], gbuf.at[c], loc_sem.at[12]),
        pltpu.make_async_copy(up_hbm.at[0], ubuf.at[c], loc_sem.at[13]),
        pltpu.make_async_copy(down_hbm.at[0], dbuf.at[c], loc_sem.at[14]),
    ]
    caches = [
        pltpu.make_async_copy(ck_hbm, kbuf, loc_sem.at[15]),
        pltpu.make_async_copy(cv_hbm, vbuf, loc_sem.at[16]),
    ]
    for copy in small + experts + caches:
        copy.start()
    for copy in small:
        copy.wait()
    wqkv[...] = jnp.concatenate(
        [
            wq_ref[...].astype(F32),
            wk_ref[...].astype(F32),
            wv_ref[...].astype(F32),
            jnp.zeros((4, 256), F32),
        ],
        axis=0,
    ).astype(BF)
    wz[z] = wqkv[...]
    wos[...] = wo_ref[...]
    woz[z] = wo_ref[...]
    stream = res_ref[...].astype(F32)
    own_squares = jnp.broadcast_to(jnp.sum(stream * stream, axis=1, keepdims=True), (16, 128))
    sqs[...] = own_squares
    mgs[...] = jnp.broadcast_to(mgain_ref[...].astype(F32).reshape(1, 256), (8, 256))

    groups = lax.shift_right_logical(ridt_ref[0:1, :], 3).astype(F32)
    grow = jnp.broadcast_to(groups, (16, 16))
    eye = (iota((16, 16), 0) == iota((16, 16), 1)).astype(F32)
    gcol = nt(eye, grow)
    before = jnp.logical_and(grow == gcol, iota((16, 16), 0) < iota((16, 16), 1))
    rank = jnp.sum(jnp.where(before, 1.0, 0.0), axis=0, keepdims=True)
    slot = groups * SLOTS + rank
    dispatch = jnp.where(iota((32, 16), 0).astype(F32) == slot, 1.0, 0.0)
    combine = nt(eye, dispatch)
    logits = logitst_ref[...]
    exps = jnp.exp(logits - jnp.max(logits, axis=0, keepdims=True))
    gates = exps / jnp.sum(exps, axis=0, keepdims=True)
    members = jnp.zeros((128, 16), F32)
    for k in range(CHOSEN):
        member = jnp.bitwise_and(ridt_ref[k : k + 1, :], GROUP_SIZE - 1)
        members = members + jnp.where(iota((128, 16), 0) == member, gates[k : k + 1, :], 0.0)
    slot_gates = lax.dot_general(
        dispatch, members, (((1,), (1,)), ((), ())), precision=lax.Precision.HIGHEST,
        preferred_element_type=F32,
    )
    for k in range(NZ):
        gz_s[k] = slot_gates[2 * k : 2 * k + 2]
    gz_r[z] = gz_s[z]

    row = iota((1024, 256), 0)
    col = iota((1024, 256), 1)
    src_g = lax.shift_right_logical(row, 7)
    src_z = jnp.bitwise_and(lax.shift_right_logical(row, 4), 7)
    src_r = jnp.bitwise_and(row, 15)
    to_query = jnp.logical_and(src_r < 8, jnp.bitwise_and(col, 63) == src_g * 8 + src_r)
    ebuf[:, 0:256] = jnp.where(to_query, 1.0, 0.0).astype(BF)
    spot = src_z * 16 + src_g * 2
    to_key = jnp.logical_and(
        jnp.logical_and(src_r >= 8, src_r < 10), col == spot + src_r - 8
    )
    to_value = jnp.logical_and(
        jnp.logical_and(src_r >= 10, src_r < 12), col == 128 + spot + src_r - 10
    )
    ebuf[:, 256:512] = jnp.where(jnp.logical_or(to_key, to_value), 1.0, 0.0).astype(BF)

    lane = iota((8, 128), 1)
    sub = iota((8, 128), 0)
    r_of = jnp.bitwise_and(lane, 15)
    place = jnp.zeros((8, 128), F32)
    for s in range(OWN):
        place = jnp.where(
            jnp.bitwise_and(sub, 3) == s, lens_ref[y * OWN + s].astype(F32), place
        )
    for k in range(NG):
        at_query = (k % (NG // 2)) * 8 + jnp.bitwise_and(r_of, 7)
        at_key = jnp.bitwise_and(lax.shift_right_logical(lane, 4), 1) * 16 + k * 2 + (
            jnp.bitwise_and(r_of, 1)
        )
        entry = jnp.where(r_of < 8, at_query, at_key).astype(F32)
        angle = place * jnp.exp(entry * (-math.log(rotary_base) / (HEAD_DIM // 2)))
        cosb[k] = jnp.cos(angle)
        sinb[k] = jnp.sin(angle)

    pl.semaphore_wait(barrier, NZ - 1 + NP - 1)

    @pl.loop(1, NY)
    def _(k):
        dev = {"tp": lax.rem(y + k, NY)}
        to(sqs, sqr.at[y], s_sq, r_sq, dev)
        to(mgs, mga.at[y], s_mg, r_mg, dev)

    @pl.loop(0, NZ - 1)
    def _(k):
        to(wqkv, wz.at[z], s_wz, r_wz, {"ep_0": lax.rem(z + far_first(k, NZ), NZ)})

    sqr[y] = own_squares
    mga[y] = mgs[...]
    drain(sqr.at[pl.ds(0, NY - 1)], r_sq)
    squares = sqr[0] + sqr[1] + sqr[2] + sqr[3]
    scale = lax.rsqrt(squares[:, 0:1] / WIDTH + norm_eps)
    normed = (stream * scale * again_ref[...].astype(F32).reshape(1, 256)).astype(BF)
    nall[g] = normed

    @pl.loop(1, NG)
    def _(k):
        other = lax.rem(g + k, NG)
        to(
            nall.at[g], nall.at[g], s_na, r_na,
            {"ep_1": lax.div(other, NC), "ep_2": lax.rem(other, NC)},
        )

    @pl.loop(0, NZ - 1)
    def _(k):
        dest = lax.rem(z + far_first(k, NZ), NZ)
        to(wos, woz.at[z], s_wo, r_wo, {"ep_0": dest})
        to(gz_s.at[dest], gz_r.at[z], s_gz, r_gz, {"ep_0": dest})

    partner = {"ep_2": 1 - c}
    for k, ref in enumerate((gbuf, ubuf, dbuf)):
        experts[k].wait()
        to(ref.at[c], ref.at[c], s_ew.at[k], r_ew.at[k], partner)

    drain(nall.at[pl.ds(0, NG - 1)], r_na)
    drain(wz.at[pl.ds(0, NZ - 1)], r_wz)
    partial = nt(nall[...].reshape(128, 256), wz[...].reshape(256, 256))
    for k in range(NP):
        sb[k, 0:4, :] = partial[4 * k : 4 * k + 4, 0:128]
        sb[k, 4:8, :] = partial[4 * k : 4 * k + 4, 128:256]

    @pl.loop(1, NP)
    def _(k):
        other = lax.rem(p + k, NP)
        to(sb.at[other], rb.at[p], s_rb, r_rb, plane_id(other))

    rb[p] = sb[p]

    drain(woz.at[pl.ds(0, NZ - 1)], r_wo)
    drain(gz_r.at[pl.ds(0, NZ - 1)], r_gz)
    for k in range(NZ):
        gown[2 * k : 2 * k + 2, :] = gz_r[k]
    gall[x] = gown[...]
    woa[:, g] = woz[...]

    @pl.loop(1, NG)
    def _(k):
        other = lax.rem(g + k, NG)
        dev = {"ep_1": lax.div(other, NC), "ep_2": lax.rem(other, NC)}
        to(woz, woa.at[:, g], s_woa, r_woa, dev)

    @pl.loop(1, NX)
    def _(k):
        to(gown, gall.at[x], s_ga, r_ga, {"ep_1": lax.rem(x + k, NX)})

    drain(rb.at[pl.ds(0, NP - 1)], r_rb)
    parts = rb[...].reshape(NG, NY, 8, 128)
    raw = parts[:, 0] + parts[:, 1] + parts[:, 2] + parts[:, 3]
    is_query = r_of < 8
    is_key = jnp.logical_and(r_of >= 8, r_of < 10)
    low_key = jnp.bitwise_and(lane, 63) < 32
    turned = []
    for k in range(NG):
        own = raw[k]
        pair = raw[(k + NG // 2) % NG]
        if k < NG // 2:
            pair = -pair
        above = pltpu.roll(own, 96, 1)
        below = pltpu.roll(own, 32, 1)
        key_pair = jnp.where(low_key, -above, below)
        spun = own * cosb[k] + jnp.where(is_query, pair, key_pair) * sinb[k]
        turned.append(jnp.where(jnp.logical_or(is_query, is_key), spun, own))
    rows8 = jnp.concatenate([t.astype(BF) for t in turned], axis=1)
    placed = nn(rows8, ebuf[:, 256:512])
    kvs[...] = placed
    kvr[y] = placed

    @pl.loop(1, NY)
    def _(k):
        to(kvs, kvr.at[y], s_kv, r_kv, {"tp": lax.rem(y + k, NY)})

    own_keys = jnp.concatenate([placed[0:4, 0:128], placed[4:8, 0:128]], axis=1)
    own_values = jnp.concatenate([placed[0:4, 128:256], placed[4:8, 128:256]], axis=1)

    pieces = []
    for s in range(OWN):
        for m in range(2):
            keep = jnp.logical_and(
                is_query,
                lax.shift_right_logical(lane, 4) == jnp.bitwise_and(2 * sub + m, 7),
            )
            line = []
            for k in range(NG):
                low = jnp.broadcast_to(turned[k][s : s + 1, :], (8, 128))
                high = jnp.broadcast_to(turned[k][4 + s : 5 + s, :], (8, 128))
                line.append(jnp.where(keep, jnp.where(sub < 4, low, high), 0.0))
            pieces.append(jnp.concatenate(line, axis=1))
    spread = nn(jnp.concatenate(pieces, axis=0).astype(BF), ebuf[:, 0:256])
    for copy in caches:
        copy.wait()
    blk = lax.shift_right_logical(iota((16, 256), 1), 6)
    row16 = iota((16, 256), 0)
    own_block = (
        lax.shift_right_logical(jnp.bitwise_and(row16, 7), 2) * 2 + lax.shift_right_logical(row16, 3)
    )
    head_low = jnp.bitwise_and(iota((16, 128), 0), 7) < 4
    lam = jnp.zeros((8, 128), F32)
    for h in range(HEADS):
        lam = jnp.where(sub == h, lam_ref[h], lam)
    for s in range(OWN):
        queries = jnp.where(blk == own_block, spread[16 * s : 16 * s + 16], 0.0)
        scores = nt(queries.astype(BF), kbuf[s]) * 0.125
        length = lens_ref[y * OWN + s]
        scores = jnp.where(iota((16, CACHE), 1) < length, scores, masked_score)
        fresh = jnp.sum(queries * own_keys[s : s + 1], axis=1, keepdims=True) * 0.125
        top = jnp.maximum(jnp.max(scores, axis=1, keepdims=True), fresh)
        weights = jnp.exp(scores - top).astype(BF)
        fresh_weight = jnp.exp(fresh - top).astype(BF).astype(F32)
        total = jnp.sum(weights.astype(F32), axis=1, keepdims=True) + fresh_weight
        mixed = nn(weights, vbuf[s])
        values = jnp.where(
            head_low,
            mixed[:, 0:128] + fresh_weight * own_values[s : s + 1, 0:128],
            mixed[:, 128:256] + fresh_weight * own_values[s : s + 1, 128:256],
        )
        averaged = values / total
        contrast = averaged[0:8] - lam * averaged[8:16]
        contrast = (
            contrast
            * lax.rsqrt(jnp.mean(contrast * contrast, axis=1, keepdims=True) + head_eps)
            * hgain_ref[...].reshape(1, 128)
        )
        rounded = contrast.astype(BF).astype(F32)
        for h in range(HEADS):
            hb[h // 2, h % 2, s : s + 1, :] = rounded[h : h + 1, :]

    hr[y] = hb[y]

    @pl.loop(1, NY)
    def _(k):
        other = lax.rem(y + k, NY)
        to(hb.at[other], hr.at[y], s_h, r_h, {"tp": other})

    drain(woa.at[:, pl.ds(0, NG - 1)], r_woa)
    drain(hr.at[pl.ds(0, NY - 1)], r_h)
    for k in range(NY):
        lhs[4 * k : 4 * k + 4, 0:128] = hr[k, 0]
        lhs[4 * k : 4 * k + 4, 128:256] = hr[k, 1]
    projected = nt(lhs[0:16].astype(BF), woa[...].reshape(WIDTH, 256))
    for k in range(NY):
        ob[k] = projected[:, 256 * k : 256 * k + 256]

    @pl.loop(1, NY)
    def _(k):
        other = lax.rem(y + k, NY)
        to(ob.at[other], orr.at[y], s_o, r_o, {"tp": other})

    orr[y] = ob[y]
    drain(orr.at[pl.ds(0, NY - 1)], r_o)
    attended = orr[0] + orr[1] + orr[2] + orr[3]
    middle = (stream + attended).astype(BF)

    routed = nn(dispatch.astype(BF), middle)
    for k in range(NZ):
        ds[k] = routed[2 * k : 2 * k + 2].astype(ds.dtype)
    dr[z] = ds[z]

    @pl.loop(0, NZ - 1)
    def _(k):
        dest = lax.rem(z + far_first(k, NZ), NZ)
        to(ds.at[dest], dr.at[z], s_d, r_d, {"ep_0": dest})

    drain(dr.at[pl.ds(0, NZ - 1)], r_d)
    for k in range(NZ):
        lhs[2 * k : 2 * k + 2, :] = dr[k].astype(F32)
    xb[x, y] = lhs[...].astype(BF)

    @pl.loop(1, NX * NY)
    def _(k):
        other = lax.rem(q16 + k, NX * NY)
        to(
            xb.at[x, y], xb.at[x, y], s_x, r_x,
            {"ep_1": lax.div(other, NY), "tp": lax.rem(other, NY)},
        )

    drain(gall.at[pl.ds(0, NX - 1)], r_ga)
    drain(mga.at[pl.ds(0, NY - 1)], r_mg)
    for k, ref in enumerate((gbuf, ubuf, dbuf)):
        drain(ref.at[0], r_ew.at[k])
    drain(fr.at[pl.ds(0, NX * NY - 1)], r_x)

    rows = NX * 32
    wide = [xb[:, k].reshape(rows, 256).astype(F32) for k in range(NY)]
    total_sq = jnp.zeros((rows, 1), F32)
    for k in range(NY):
        total_sq = total_sq + jnp.sum(wide[k] * wide[k], axis=1, keepdims=True)
    scale = lax.rsqrt(total_sq / WIDTH + norm_eps)
    mixed_in = [(wide[k] * scale * mga[k, 0:1, :]).astype(BF) for k in range(NY)]
    produced = jnp.zeros((rows, WIDTH), F32)
    for e in range(NC):
        gate_act = jnp.zeros((rows, 128), F32)
        up_act = jnp.zeros((rows, 128), F32)
        for k in range(NY):
            gate_act = gate_act + nn(mixed_in[k], gbuf[e, 256 * k : 256 * k + 256, :])
            up_act = up_act + nn(mixed_in[k], ubuf[e, 256 * k : 256 * k + 256, :])
        hidden = (gate_act / (1.0 + jnp.exp(-gate_act)) * up_act).astype(BF)
        slot_gate = jnp.sum(
            jnp.where(iota((rows, 128), 1) == x * NC + e, gall[...].reshape(rows, 128), 0.0),
            axis=1,
            keepdims=True,
        )
        produced = produced + nn(hidden, dbuf[e]) * slot_gate

    for k in range(NX):
        for j in range(NY):
            fs[k, j] = produced[32 * k : 32 * k + 32, 256 * j : 256 * j + 256].astype(BF)

    @pl.loop(1, NX * NY)
    def _(k):
        other = lax.rem(q16 + k, NX * NY)
        ox, oy = lax.div(other, NY), lax.rem(other, NY)
        to(fs.at[ox, oy], fr.at[q16], s_f, r_f, {"ep_1": ox, "tp": oy})

    fr[q16] = fs[x, y]
    drain(fr.at[pl.ds(0, NX * NY - 1)], r_f)
    mixture = fr[0].astype(F32)
    for k in range(1, NX * NY):
        mixture = mixture + fr[k].astype(F32)
    for k in range(NZ):
        zs[k] = mixture[2 * k : 2 * k + 2].astype(zs.dtype)
    zr[z] = zs[z]

    @pl.loop(0, NZ - 1)
    def _(k):
        dest = lax.rem(z + far_first(k, NZ), NZ)
        to(zs.at[dest], zr.at[z], s_z, r_z, {"ep_0": dest})

    drain(kvr.at[pl.ds(0, NY - 1)], r_kv)
    for k in range(NY):
        for half in range(2):
            kvo[4 * k : 4 * k + 4, 128 * half : 128 * half + 128] = kvr[k, 4 * half : 4 * half + 4, 0:128]
            kvo[4 * k : 4 * k + 4, 256 + 128 * half : 384 + 128 * half] = kvr[
                k, 4 * half : 4 * half + 4, 128:256
            ]
    out_ref[1] = kvo[:, 0:256].astype(BF)
    out_ref[2] = kvo[:, 256:512].astype(BF)

    drain(zr.at[pl.ds(0, NZ - 1)], r_z)
    for k in range(NZ):
        lhs[2 * k : 2 * k + 2, :] = zr[k].astype(F32)
    mix = nn(combine.astype(BF), lhs[...].astype(BF))
    out_ref[0] = (middle.astype(F32) + mix).astype(BF)

    for ref, sem in (
        (wz, s_wz),
        (woz, s_wo),
        (gz_r, s_gz),
        (dr, s_d),
        (zr, s_z),
    ):
        drain(ref.at[pl.ds(0, NZ - 1)], sem)
    for ref, sem in ((sqr, s_sq), (mga, s_mg), (kvr, s_kv), (hr, s_h), (orr, s_o)):
        drain(ref.at[pl.ds(0, NY - 1)], sem)
    drain(nall.at[pl.ds(0, NG - 1)], s_na)
    drain(gall.at[pl.ds(0, NX - 1)], s_ga)
    for k, ref in enumerate((gbuf, ubuf, dbuf)):
        drain(ref.at[0], s_ew.at[k])
    drain(woa.at[:, pl.ds(0, NG - 1)], s_woa)
    drain(rb.at[pl.ds(0, NP - 1)], s_rb)
    drain(fr.at[pl.ds(0, NX * NY - 1)], s_x)
    drain(fr.at[pl.ds(0, NX * NY - 1)], s_f)


def on_device(
    residual,
    cache_keys,
    cache_values,
    lengths,
    query_weight,
    key_weight,
    value_weight,
    out_weight,
    head_gain,
    mix_lambda,
    attn_gain,
    moe_gain,
    route_ids,
    route_logits,
    gate_weight,
    up_weight,
    down_weight,
):
    vm = pl.BlockSpec(memory_space=pltpu.VMEM)
    hbm = pl.BlockSpec(memory_space=pl.ANY)
    dma = pltpu.SemaphoreType.DMA
    V = pltpu.VMEM
    scratch = [
        V((16, 256), BF),
        pltpu.SMEM((16,), jnp.int32),
        V((8, 256), BF),
        V((2, 256), BF),
        V((2, 256), BF),
        V((8, 256), BF),
        V((128,), F32),
        pltpu.SMEM((HEADS,), F32),
        V((256,), BF),
        V((256,), BF),
        V((CHOSEN, 16), jnp.int32),
        V((CHOSEN, 16), F32),
        V((OWN, CACHE, 256), BF),
        V((OWN, CACHE, 256), BF),
        V((NC, WIDTH, 128), BF),
        V((NC, WIDTH, 128), BF),
        V((NC, 128, WIDTH), BF),
        dma((17,)),
        V((16, 256), BF),
        V((NZ, 16, 256), BF),
        V((8, 256), BF),
        V((NZ, 8, 256), BF),
        V((NZ, NG, 8, 256), BF),
        V((16, 128), F32),
        V((NY, 16, 128), F32),
        V((NG, 16, 256), BF),
        V((8, 256), F32),
        V((NY, 8, 256), F32),
        V((NP, 8, 128), F32),
        V((NP, 8, 128), F32),
        V((1024, 512), BF),
        V((NG, 8, 128), F32),
        V((NG, 8, 128), F32),
        V((8, 256), F32),
        V((NY, 8, 256), F32),
        V((16, 512), F32),
        V((NY, 2, OWN, 128), F32),
        V((NY, 2, OWN, 128), F32),
        V((32, 256), F32),
        V((NY, 16, 256), F32),
        V((NY, 16, 256), F32),
        V((NZ, SLOTS, 128), F32),
        V((NZ, SLOTS, 128), F32),
        V((32, 128), F32),
        V((NX, 32, 128), F32),
        V((NZ, SLOTS, 256), BF),
        V((NZ, SLOTS, 256), BF),
        V((NX, NY, 32, 256), BF),
        V((NX, NY, 32, 256), BF),
        V((NX * NY, 32, 256), BF),
        V((NZ, SLOTS, 256), BF),
        V((NZ, SLOTS, 256), BF),
    ]
    sems = [dma] * 34
    sems[28] = sems[29] = dma((3,))
    results = pl.pallas_call(
        kernel,
        out_shape=pltpu.VMEM((3, 16, 256), BF),
        in_specs=[hbm] * 17,
        out_specs=vm,
        scratch_shapes=scratch + sems,
        compiler_params=pltpu.CompilerParams(collective_id=0, has_side_effects=True),
        cost_estimate=pl.CostEstimate(flops=10**9, bytes_accessed=5 * 10**6, transcendentals=0),
    )(
        residual,
        cache_keys,
        cache_values,
        lengths,
        query_weight.T,
        key_weight.T,
        value_weight.T,
        out_weight.T,
        head_gain,
        mix_lambda,
        attn_gain,
        moe_gain,
        route_ids.T,
        route_logits.T,
        gate_weight,
        up_weight,
        down_weight,
    )
    return results[0], results[1], results[2]


def solution(mesh):
    torus = Mesh(mesh.devices.reshape(NZ, NX, NC, NY), ("ep_0", "ep_1", "ep_2", "tp"))
    return jax.shard_map(
        on_device,
        mesh=torus,
        in_specs=(
            P(EP, "tp"),
            P(EP_TP, None, None),
            P(EP_TP, None, None),
            P(EP),
            P("tp", EP),
            P("tp", EP),
            P("tp", EP),
            P("tp", EP),
            P(),
            P(),
            P("tp"),
            P("tp"),
            P(EP, None),
            P(EP, None),
            P(EP, None, "tp"),
            P(EP, None, "tp"),
            P(EP, "tp", None),
        ),
        out_specs=(P(EP, "tp"), P(EP, None), P(EP, None)),
        check_vma=False,
    )
```

```python
import math

import jax
import jax.numpy as jnp
from jax import lax
from jax.experimental import pallas as pl
from jax.experimental.pallas import tpu as pltpu
from jax.sharding import Mesh
from jax.sharding import PartitionSpec as P

WIDTH = 1024
HEADS = 8
HEAD_DIM = 64
VALUE_DIM = 128
CHOSEN = 6
GROUP_SIZE = 8
SLOTS = 2
EP = ("ep_0", "ep_1", "ep_2")
EP_TP = ("ep_0", "ep_1", "ep_2", "tp")
NZ, NX, NC, NY = 16, 4, 2, 4
NG = NX * NC
NP = NG * NY
CACHE = 1024
OWN = 4

norm_eps = 1e-06
head_eps = 1e-05
masked_score = -1e30
rotary_base = 500000.0

MESH = pl.DeviceIdType.MESH
BF = jnp.bfloat16
F32 = jnp.float32


def nt(a, b):
    return lax.dot_general(a, b, (((1,), (1,)), ((), ())), preferred_element_type=F32)


def nn(a, b):
    return lax.dot_general(a, b, (((1,), (0,)), ((), ())), preferred_element_type=F32)


def far_first(k, n):
    half = lax.div(k + 1, 2)
    return jnp.where(lax.rem(k, 2) == 1, n // 2 + half, n // 2 - half)


def iota(shape, dim):
    return lax.broadcasted_iota(jnp.int32, shape, dim)


def kernel(
    res_hbm,
    ck_hbm,
    cv_hbm,
    lens_hbm,
    wq_hbm,
    wk_hbm,
    wv_hbm,
    wo_hbm,
    hgain_hbm,
    lam_hbm,
    again_hbm,
    mgain_hbm,
    ridt_hbm,
    logitst_hbm,
    gate_hbm,
    up_hbm,
    down_hbm,
    out_ref,
    res_ref,
    lens_ref,
    wq_ref,
    wk_ref,
    wv_ref,
    wo_ref,
    hgain_ref,
    lam_ref,
    again_ref,
    mgain_ref,
    ridt_ref,
    logitst_ref,
    kbuf,
    vbuf,
    gbuf,
    ubuf,
    dbuf,
    loc_sem,
    wkv,
    wzq,
    wzk,
    woy,
    woa,
    sqs,
    sqr,
    nall,
    mgs,
    mga,
    sb,
    rb,
    ebuf,
    cosb,
    sinb,
    kvs,
    kvr,
    kvo,
    hb,
    hr,
    heads,
    lhs,
    gz_s,
    gz_r,
    gown,
    gall,
    ds,
    dr,
    xb,
    fs,
    fr,
    zs,
    zr,
    s_wzq,
    r_wzq,
    s_wzk,
    r_wzk,
    s_wo,
    r_wo,
    s_woa,
    r_woa,
    s_sq,
    r_sq,
    s_na,
    r_na,
    s_mg,
    r_mg,
    s_rb,
    r_rb,
    s_kv,
    r_kv,
    s_h,
    r_h,
    s_woc,
    r_woc,
    s_gz,
    r_gz,
    s_ga,
    r_ga,
    s_d,
    r_d,
    s_x,
    r_x,
    s_ew,
    r_ew,
    s_f,
    r_f,
    s_z,
    r_z,
):
    z = lax.axis_index("ep_0")
    x = lax.axis_index("ep_1")
    c = lax.axis_index("ep_2")
    y = lax.axis_index("tp")
    g = x * NC + c
    p = g * NY + y
    twin = x * NC + 1 - c
    q16 = x * NY + y

    def plane_id(other):
        og = lax.div(other, NY)
        return {"ep_1": lax.div(og, NC), "ep_2": lax.rem(og, NC), "tp": lax.rem(other, NY)}

    def along_z(k):
        dest = lax.rem(z + far_first(k, NZ), NZ)
        return dest, {"ep_0": dest, "ep_2": 1 - c}

    def to(src, dst, ssem, rsem, dev):
        pltpu.make_async_remote_copy(
            src_ref=src, dst_ref=dst, send_sem=ssem, recv_sem=rsem, device_id=dev, device_id_type=MESH
        ).start()

    def drain(ref, sem):
        pltpu.make_async_copy(ref, ref, sem).wait()

    barrier = pltpu.get_barrier_semaphore()

    @pl.loop(0, NZ - 1)
    def _(k):
        pl.semaphore_signal(barrier, inc=1, device_id=along_z(k)[1], device_id_type=MESH)

    @pl.loop(0, 4)
    def _(k):
        source = 4 * y + k

        @pl.when(source != z)
        def _():
            @pl.loop(1, NY)
            def _(j):
                dev = {"ep_0": source, "ep_2": 1 - c, "tp": lax.rem(y + j, NY)}
                pl.semaphore_signal(barrier, inc=1, device_id=dev, device_id_type=MESH)

    @pl.loop(1, NP)
    def _(k):
        pl.semaphore_signal(
            barrier, inc=1, device_id=plane_id(lax.rem(p + k, NP)), device_id_type=MESH
        )

    small = [
        pltpu.make_async_copy(src, dst, loc_sem.at[k])
        for k, (src, dst) in enumerate(
            (
                (res_hbm, res_ref),
                (wq_hbm, wq_ref),
                (wk_hbm, wk_ref),
                (wv_hbm, wv_ref),
                (wo_hbm, wo_ref),
                (mgain_hbm, mgain_ref),
                (again_hbm, again_ref),
                (hgain_hbm, hgain_ref),
                (ridt_hbm, ridt_ref),
                (logitst_hbm, logitst_ref),
                (lens_hbm, lens_ref),
                (lam_hbm, lam_ref),
            )
        )
    ]
    experts = [
        pltpu.make_async_copy(gate_hbm.at[0], gbuf.at[c], loc_sem.at[12]),
        pltpu.make_async_copy(up_hbm.at[0], ubuf.at[c], loc_sem.at[13]),
        pltpu.make_async_copy(down_hbm.at[0], dbuf.at[c], loc_sem.at[14]),
    ]
    caches = [
        pltpu.make_async_copy(ck_hbm, kbuf, loc_sem.at[15]),
        pltpu.make_async_copy(cv_hbm, vbuf, loc_sem.at[16]),
    ]
    for copy in small + experts + caches:
        copy.start()
    for copy in small:
        copy.wait()
    wkv[...] = jnp.concatenate([wk_ref[...].astype(F32), wv_ref[...].astype(F32)], axis=0).astype(BF)
    stream = res_ref[...].astype(F32)
    own_squares = jnp.broadcast_to(jnp.sum(stream * stream, axis=1, keepdims=True), (16, 128))
    sqs[...] = own_squares
    mgs[...] = jnp.broadcast_to(mgain_ref[...].astype(F32).reshape(1, 256), (8, 256))

    groups = lax.shift_right_logical(ridt_ref[0:1, :], 3).astype(F32)
    grow = jnp.broadcast_to(groups, (16, 16))
    eye = (iota((16, 16), 0) == iota((16, 16), 1)).astype(F32)
    gcol = nt(eye, grow)
    before = jnp.logical_and(grow == gcol, iota((16, 16), 0) < iota((16, 16), 1))
    rank = jnp.sum(jnp.where(before, 1.0, 0.0), axis=0, keepdims=True)
    slot = groups * SLOTS + rank
    dispatch = jnp.where(iota((32, 16), 0).astype(F32) == slot, 1.0, 0.0)
    combine = nt(eye, dispatch)
    logits = logitst_ref[...]
    exps = jnp.exp(logits - jnp.max(logits, axis=0, keepdims=True))
    gates = exps / jnp.sum(exps, axis=0, keepdims=True)
    members = jnp.zeros((128, 16), F32)
    for k in range(CHOSEN):
        member = jnp.bitwise_and(ridt_ref[k : k + 1, :], GROUP_SIZE - 1)
        members = members + jnp.where(iota((128, 16), 0) == member, gates[k : k + 1, :], 0.0)
    slot_gates = lax.dot_general(
        dispatch, members, (((1,), (1,)), ((), ())), precision=lax.Precision.HIGHEST,
        preferred_element_type=F32,
    )
    for k in range(NZ):
        gz_s[k] = slot_gates[2 * k : 2 * k + 2]

    row = iota((1024, 256), 0)
    col = iota((1024, 256), 1)
    src_g = jnp.bitwise_xor(lax.shift_right_logical(row, 7), 1)
    src_lane = jnp.bitwise_and(row, 127)
    to_query = jnp.bitwise_and(col, 63) == src_g * 8 + jnp.bitwise_and(src_lane, 7)
    ebuf[:, 0:256] = jnp.where(to_query, 1.0, 0.0).astype(BF)
    src_r = jnp.bitwise_and(src_lane, 3)
    spot = lax.shift_right_logical(src_lane, 2) * 16 + src_g * 2 + jnp.bitwise_and(src_r, 1)
    on_spot = jnp.logical_and(col == spot, src_lane < 64)
    ebuf[:, 256:512] = jnp.where(jnp.logical_and(on_spot, src_r < 2), 1.0, 0.0).astype(BF)
    ebuf[:, 512:768] = jnp.where(jnp.logical_and(on_spot, src_r >= 2), 1.0, 0.0).astype(BF)

    lane = iota((8, 128), 1)
    sub = iota((8, 128), 0)
    place = jnp.zeros((8, 128), F32)
    for s in range(OWN):
        place = jnp.where(
            jnp.bitwise_and(sub, 3) == s, lens_ref[y * OWN + s].astype(F32), place
        )
    for k in range(NG):
        at_query = ((k ^ 1) % (NG // 2)) * 8 + jnp.bitwise_and(lane, 7)
        at_key = (
            jnp.bitwise_and(lax.shift_right_logical(lane, 2), 1) * 16
            + (k ^ 1) * 2
            + jnp.bitwise_and(lane, 1)
        )
        entry = jnp.where(sub < 4, at_query, at_key).astype(F32)
        angle = place * jnp.exp(entry * (-math.log(rotary_base) / (HEAD_DIM // 2)))
        cosb[k] = jnp.cos(angle)
        sinb[k] = jnp.sin(angle)

    quarter = lax.div(z, 4)
    pl.semaphore_wait(barrier, NZ - 1 + NP - 1 + jnp.where(quarter == y, 0, NZ - 1))

    @pl.loop(1, NY)
    def _(k):
        dev = {"tp": lax.rem(y + k, NY)}
        to(sqs, sqr.at[y], s_sq, r_sq, dev)
        to(mgs, mga.at[y], s_mg, r_mg, dev)

    @pl.loop(0, NZ)
    def _(k):
        dev = along_z(k)[1]
        to(wq_ref, wzq.at[z], s_wzq, r_wzq, dev)
        to(wkv, wzk.at[z], s_wzk, r_wzk, dev)

    sqr[y] = own_squares
    mga[y] = mgs[...]
    drain(sqr.at[pl.ds(0, NY - 1)], r_sq)
    squares = sqr[0] + sqr[1] + sqr[2] + sqr[3]
    scale = lax.rsqrt(squares[:, 0:1] / WIDTH + norm_eps)
    normed = (stream * scale * again_ref[...].astype(F32).reshape(1, 256)).astype(BF)
    nall[g] = normed

    @pl.loop(1, NG)
    def _(k):
        other = lax.rem(g + k, NG)
        to(
            nall.at[g], nall.at[g], s_na, r_na,
            {"ep_1": lax.div(other, NC), "ep_2": lax.rem(other, NC)},
        )

    @pl.loop(0, NZ)
    def _(k):
        dest, dev = along_z(k)
        wo_dev = {"ep_0": dest, "ep_2": 1 - c, "tp": quarter}
        to(wo_ref, woy.at[y, lax.rem(z, 4)], s_wo, r_wo, wo_dev)
        to(gz_s.at[dest], gz_r.at[k], s_gz, r_gz, dev)

    partner = {"ep_2": 1 - c}
    for k, ref in enumerate((gbuf, ubuf, dbuf)):
        experts[k].wait()
        to(ref.at[c], ref.at[c], s_ew.at[k], r_ew.at[k], partner)

    drain(nall.at[pl.ds(0, NG - 1)], r_na)
    drain(wzq, r_wzq)
    drain(wzk, r_wzk)
    tokens = nall[...].reshape(128, 256)
    part_q = nt(tokens, wzq[...].reshape(128, 256))
    part_kv = nt(tokens, wzk[...].reshape(64, 256))
    part_kv = jnp.concatenate([part_kv, jnp.zeros((128, 64), F32)], axis=1)
    for k in range(NP):
        sb[k, 0:4, :] = part_q[4 * k : 4 * k + 4]
        sb[k, 4:8, :] = part_kv[4 * k : 4 * k + 4]

    @pl.loop(1, NP)
    def _(k):
        other = lax.rem(p + k, NP)
        to(sb.at[other], rb.at[p], s_rb, r_rb, plane_id(other))

    rb[p] = sb[p]

    drain(gz_r, r_gz)
    for k in range(NZ):
        gown[2 * k : 2 * k + 2, :] = gz_r[k]
    gall[x] = gown[...]

    @pl.loop(1, NX)
    def _(k):
        to(gown, gall.at[x], s_ga, r_ga, {"ep_1": lax.rem(x + k, NX)})

    drain(woy, r_wo)
    woa[:, :, twin] = woy[...]
    to(woy, woa.at[:, :, twin], s_woc, r_woc, partner)

    @pl.loop(1, NX)
    def _(k):
        to(woy, woa.at[:, :, twin], s_woa, r_woa, {"ep_1": lax.rem(x + k, NX)})

    drain(rb.at[pl.ds(0, NP - 1)], r_rb)
    parts = rb[...].reshape(NG, NY, 8, 128)
    raw = parts[:, 0] + parts[:, 1] + parts[:, 2] + parts[:, 3]
    is_query = sub < 4
    is_key = jnp.logical_and(lane < 64, jnp.bitwise_and(lane, 3) < 2)
    low_key = jnp.bitwise_and(lane, 15) < 8
    turned = []
    for k in range(NG):
        own = raw[k]
        pair = raw[(k + NG // 2) % NG]
        if k < NG // 2:
            pair = -pair
        above = pltpu.roll(own, 120, 1)
        below = pltpu.roll(own, 8, 1)
        key_pair = jnp.where(low_key, -above, below)
        spun = own * cosb[k] + jnp.where(is_query, pair, key_pair) * sinb[k]
        turned.append(jnp.where(jnp.logical_or(is_query, is_key), spun, own))
    rows8 = jnp.concatenate([t.astype(BF) for t in turned], axis=1)
    placed = nn(rows8, ebuf[:, 256:768])
    kvs[...] = placed
    kvr[y] = placed

    @pl.loop(1, NY)
    def _(k):
        to(kvs, kvr.at[y], s_kv, r_kv, {"tp": lax.rem(y + k, NY)})

    own_keys = placed[4:8, 0:256]
    own_values = placed[4:8, 256:512]

    pieces = []
    for s in range(OWN):
        for m in range(2):
            keep = lax.shift_right_logical(lane, 3) == 2 * sub + m
            line = []
            for k in range(NG):
                whole = jnp.broadcast_to(turned[k][s : s + 1, :], (8, 128))
                line.append(jnp.where(keep, whole, 0.0))
            pieces.append(jnp.concatenate(line, axis=1))
    spread = nn(jnp.concatenate(pieces, axis=0).astype(BF), ebuf[:, 0:256])
    for copy in caches:
        copy.wait()
    blk = lax.shift_right_logical(iota((16, 256), 1), 6)
    row16 = iota((16, 256), 0)
    own_block = (
        lax.shift_right_logical(jnp.bitwise_and(row16, 7), 2) * 2 + lax.shift_right_logical(row16, 3)
    )
    head_low = jnp.bitwise_and(iota((16, 128), 0), 7) < 4
    lam = jnp.zeros((8, 128), F32)
    for h in range(HEADS):
        lam = jnp.where(sub == h, lam_ref[h], lam)
    for s in range(OWN):
        queries = jnp.where(blk == own_block, spread[16 * s : 16 * s + 16], 0.0)
        scores = nt(queries.astype(BF), kbuf[s]) * 0.125
        length = lens_ref[y * OWN + s]
        scores = jnp.where(iota((16, CACHE), 1) < length, scores, masked_score)
        fresh = jnp.sum(queries * own_keys[s : s + 1], axis=1, keepdims=True) * 0.125
        top = jnp.maximum(jnp.max(scores, axis=1, keepdims=True), fresh)
        weights = jnp.exp(scores - top).astype(BF)
        fresh_weight = jnp.exp(fresh - top).astype(BF).astype(F32)
        total = jnp.sum(weights.astype(F32), axis=1, keepdims=True) + fresh_weight
        mixed = nn(weights, vbuf[s])
        values = jnp.where(
            head_low,
            mixed[:, 0:128] + fresh_weight * own_values[s : s + 1, 0:128],
            mixed[:, 128:256] + fresh_weight * own_values[s : s + 1, 128:256],
        )
        averaged = values / total
        contrast = averaged[0:8] - lam * averaged[8:16]
        contrast = (
            contrast
            * lax.rsqrt(jnp.mean(contrast * contrast, axis=1, keepdims=True) + head_eps)
            * hgain_ref[...].reshape(1, 128)
        )
        rounded = contrast.astype(BF).astype(F32)
        for h in range(HEADS):
            hb[h, s : s + 1, :] = rounded[h : h + 1, :]

    hr[y] = hb[...]

    @pl.loop(1, NY)
    def _(k):
        to(hb, hr.at[y], s_h, r_h, {"tp": lax.rem(y + k, NY)})

    drain(woa.at[:, :, pl.ds(0, NX - 1)], r_woa)

    @pl.loop(1, NX)
    def _(k):
        block = woa.at[:, :, lax.rem(x + k, NX) * NC + 1 - c]
        to(block, block, s_woc, r_woc, partner)

    drain(hr.at[pl.ds(0, NY - 1)], r_h)
    drain(woa.at[:, :, pl.ds(0, NX)], r_woc)
    for k in range(NY):
        for h in range(HEADS):
            heads[4 * k : 4 * k + 4, 128 * h : 128 * h + 128] = hr[k, h]
    lined = heads[...].astype(BF)
    attended = jnp.zeros((16, 256), F32)
    for k in range(NY):
        attended = attended + nt(lined[:, 256 * k : 256 * k + 256], woa[k].reshape(256, 256))
    middle = (stream + attended).astype(BF)

    routed = nn(dispatch.astype(BF), middle)
    for k in range(NZ):
        ds[k] = routed[2 * k : 2 * k + 2].astype(ds.dtype)

    @pl.loop(0, NZ)
    def _(k):
        dest, dev = along_z(k)
        to(ds.at[dest], dr.at[k], s_d, r_d.at[lax.div(k, 8)], dev)

    rows = NX * 16

    def spread(b):
        drain(dr.at[pl.ds(8 * b, 8)], r_d.at[b])
        for k in range(8):
            lhs[2 * k : 2 * k + 2, :] = dr[8 * b + k].astype(F32)
        xb[b, x, y] = lhs[0:16].astype(BF)

        @pl.loop(1, NX * NY)
        def _(k):
            other = lax.rem(q16 + k, NX * NY)
            to(
                xb.at[b, x, y], xb.at[b, x, y], s_x.at[b], r_x.at[b],
                {"ep_1": lax.div(other, NY), "tp": lax.rem(other, NY)},
            )

    def run_experts(b):
        wide = [xb[b, :, k].reshape(rows, 256).astype(F32) for k in range(NY)]
        total_sq = jnp.zeros((rows, 1), F32)
        for k in range(NY):
            total_sq = total_sq + jnp.sum(wide[k] * wide[k], axis=1, keepdims=True)
        scale = lax.rsqrt(total_sq / WIDTH + norm_eps)
        mixed_in = [(wide[k] * scale * mga[k, 0:1, :]).astype(BF) for k in range(NY)]
        member = gall[:, 16 * b : 16 * b + 16, :].reshape(rows, 128)
        produced = jnp.zeros((rows, WIDTH), F32)
        for e in range(NC):
            gate_act = jnp.zeros((rows, 128), F32)
            up_act = jnp.zeros((rows, 128), F32)
            for k in range(NY):
                gate_act = gate_act + nn(mixed_in[k], gbuf[e, 256 * k : 256 * k + 256, :])
                up_act = up_act + nn(mixed_in[k], ubuf[e, 256 * k : 256 * k + 256, :])
            hidden = (gate_act / (1.0 + jnp.exp(-gate_act)) * up_act).astype(BF)
            slot_gate = jnp.sum(
                jnp.where(iota((rows, 128), 1) == x * NC + e, member, 0.0), axis=1, keepdims=True
            )
            produced = produced + nn(hidden, dbuf[e]) * slot_gate
        for k in range(NX):
            for j in range(NY):
                fs[b, k, j] = produced[16 * k : 16 * k + 16, 256 * j : 256 * j + 256].astype(BF)

        @pl.loop(1, NX * NY)
        def _(k):
            other = lax.rem(q16 + k, NX * NY)
            ox, oy = lax.div(other, NY), lax.rem(other, NY)
            to(fs.at[b, ox, oy], fr.at[b, q16], s_f.at[b], r_f.at[b], {"ep_1": ox, "tp": oy})

        fr[b, q16] = fs[b, x, y]

    def give_back(b):
        drain(fr.at[b, pl.ds(0, NX * NY - 1)], r_f.at[b])
        mixture = fr[b, 0].astype(F32)
        for k in range(1, NX * NY):
            mixture = mixture + fr[b, k].astype(F32)
        for k in range(8):
            zs[8 * b + k] = mixture[2 * k : 2 * k + 2].astype(zs.dtype)

        @pl.loop(8 * b, 8 * b + 8)
        def _(k):
            source = lax.rem(z + 2 * NZ - far_first(k, NZ), NZ)
            to(zs.at[k], zr.at[z], s_z, r_z, {"ep_0": source, "ep_2": 1 - c})

    spread(1)
    spread(0)
    drain(gall.at[pl.ds(0, NX - 1)], r_ga)
    drain(mga.at[pl.ds(0, NY - 1)], r_mg)
    for k, ref in enumerate((gbuf, ubuf, dbuf)):
        drain(ref.at[0], r_ew.at[k])
    drain(fr.at[1, pl.ds(0, NX * NY - 1)], r_x.at[1])
    run_experts(1)
    drain(fr.at[0, pl.ds(0, NX * NY - 1)], r_x.at[0])
    run_experts(0)
    give_back(1)
    give_back(0)

    drain(kvr.at[pl.ds(0, NY - 1)], r_kv)
    for k in range(NY):
        kvo[4 * k : 4 * k + 4, :] = kvr[k, 4:8, :]
    out_ref[1] = kvo[:, 0:256].astype(BF)
    out_ref[2] = kvo[:, 256:512].astype(BF)

    drain(zr, r_z)
    for k in range(NZ):
        lhs[2 * k : 2 * k + 2, :] = zr[k].astype(F32)
    mix = nn(combine.astype(BF), lhs[...].astype(BF))
    out_ref[0] = (middle.astype(F32) + mix).astype(BF)

    for ref, sem in (
        (wzq, s_wzq),
        (wzk, s_wzk),
        (woy, s_wo),
        (gz_r, s_gz),
        (dr, s_d),
        (zr, s_z),
    ):
        drain(ref, sem)
    for ref, sem in ((sqr, s_sq), (mga, s_mg), (kvr, s_kv), (hr, s_h)):
        drain(ref.at[pl.ds(0, NY - 1)], sem)
    drain(nall.at[pl.ds(0, NG - 1)], s_na)
    drain(gall.at[pl.ds(0, NX - 1)], s_ga)
    for k, ref in enumerate((gbuf, ubuf, dbuf)):
        drain(ref.at[0], s_ew.at[k])
    drain(woa.at[:, :, pl.ds(0, NX - 1)], s_woa)
    drain(woa.at[:, :, pl.ds(0, NX)], s_woc)
    drain(rb.at[pl.ds(0, NP - 1)], s_rb)
    for b in range(2):
        drain(fr.at[b, pl.ds(0, NX * NY - 1)], s_x.at[b])
        drain(fr.at[b, pl.ds(0, NX * NY - 1)], s_f.at[b])


def on_device(
    residual,
    cache_keys,
    cache_values,
    lengths,
    query_weight,
    key_weight,
    value_weight,
    out_weight,
    head_gain,
    mix_lambda,
    attn_gain,
    moe_gain,
    route_ids,
    route_logits,
    gate_weight,
    up_weight,
    down_weight,
):
    vm = pl.BlockSpec(memory_space=pltpu.VMEM)
    hbm = pl.BlockSpec(memory_space=pl.ANY)
    dma = pltpu.SemaphoreType.DMA
    V = pltpu.VMEM
    scratch = [
        V((16, 256), BF),
        pltpu.SMEM((16,), jnp.int32),
        V((8, 256), BF),
        V((2, 256), BF),
        V((2, 256), BF),
        V((8, 256), BF),
        V((128,), F32),
        pltpu.SMEM((HEADS,), F32),
        V((256,), BF),
        V((256,), BF),
        V((CHOSEN, 16), jnp.int32),
        V((CHOSEN, 16), F32),
        V((OWN, CACHE, 256), BF),
        V((OWN, CACHE, 256), BF),
        V((NC, WIDTH, 128), BF),
        V((NC, WIDTH, 128), BF),
        V((NC, 128, WIDTH), BF),
        dma((17,)),
        V((4, 256), BF),
        V((NZ, 8, 256), BF),
        V((NZ, 4, 256), BF),
        V((NY, NZ // NY, 8, 256), BF),
        V((NY, NZ // NY, NG, 8, 256), BF),
        V((16, 128), F32),
        V((NY, 16, 128), F32),
        V((NG, 16, 256), BF),
        V((8, 256), F32),
        V((NY, 8, 256), F32),
        V((NP, 8, 128), F32),
        V((NP, 8, 128), F32),
        V((1024, 768), BF),
        V((NG, 8, 128), F32),
        V((NG, 8, 128), F32),
        V((8, 512), F32),
        V((NY, 8, 512), F32),
        V((16, 512), F32),
        V((HEADS, OWN, 128), F32),
        V((NY, HEADS, OWN, 128), F32),
        V((16, WIDTH), F32),
        V((32, 256), F32),
        V((NZ, SLOTS, 128), F32),
        V((NZ, SLOTS, 128), F32),
        V((32, 128), F32),
        V((NX, 32, 128), F32),
        V((NZ, SLOTS, 256), BF),
        V((NZ, SLOTS, 256), BF),
        V((2, NX, NY, 16, 256), BF),
        V((2, NX, NY, 16, 256), BF),
        V((2, NX * NY, 16, 256), BF),
        V((NZ, SLOTS, 256), BF),
        V((NZ, SLOTS, 256), BF),
    ]
    sems = [dma] * 36
    sems[30] = sems[31] = dma((3,))
    sems[27] = sems[28] = sems[29] = sems[32] = sems[33] = dma((2,))
    results = pl.pallas_call(
        kernel,
        out_shape=pltpu.VMEM((3, 16, 256), BF),
        in_specs=[hbm] * 17,
        out_specs=vm,
        scratch_shapes=scratch + sems,
        compiler_params=pltpu.CompilerParams(collective_id=0, has_side_effects=True),
        cost_estimate=pl.CostEstimate(flops=10**9, bytes_accessed=5 * 10**6, transcendentals=0),
    )(
        residual,
        cache_keys,
        cache_values,
        lengths,
        query_weight.T,
        key_weight.T,
        value_weight.T,
        out_weight.T,
        head_gain,
        mix_lambda,
        attn_gain,
        moe_gain,
        route_ids.T,
        route_logits.T,
        gate_weight,
        up_weight,
        down_weight,
    )
    return results[0], results[1], results[2]


def solution(mesh):
    torus = Mesh(mesh.devices.reshape(NZ, NX, NC, NY), ("ep_0", "ep_1", "ep_2", "tp"))
    return jax.shard_map(
        on_device,
        mesh=torus,
        in_specs=(
            P(EP, "tp"),
            P(EP_TP, None, None),
            P(EP_TP, None, None),
            P(EP),
            P("tp", EP),
            P("tp", EP),
            P("tp", EP),
            P("tp", EP),
            P(),
            P(),
            P("tp"),
            P("tp"),
            P(EP, None),
            P(EP, None),
            P(EP, None, "tp"),
            P(EP, None, "tp"),
            P(EP, "tp", None),
        ),
        out_specs=(P(EP, "tp"), P(EP, None), P(EP, None)),
        check_vma=False,
    )
```

```python
import math

import jax
import jax.numpy as jnp
from jax import lax
from jax.experimental import pallas as pl
from jax.experimental.pallas import tpu as pltpu
from jax.sharding import Mesh
from jax.sharding import PartitionSpec as P

WIDTH = 1024
HEADS = 8
HEAD_DIM = 64
VALUE_DIM = 128
CHOSEN = 6
GROUP_SIZE = 8
SLOTS = 2
EP = ("ep_0", "ep_1", "ep_2")
EP_TP = ("ep_0", "ep_1", "ep_2", "tp")
NZ, NX, NC, NY = 16, 4, 2, 4
NG = NX * NC
NP = NG * NY
CACHE = 1024
OWN = 4

norm_eps = 1e-06
head_eps = 1e-05
masked_score = -1e30
rotary_base = 500000.0

MESH = pl.DeviceIdType.MESH
BF = jnp.bfloat16
F32 = jnp.float32


def nt(a, b):
    return lax.dot_general(a, b, (((1,), (1,)), ((), ())), preferred_element_type=F32)


def nn(a, b):
    return lax.dot_general(a, b, (((1,), (0,)), ((), ())), preferred_element_type=F32)


def far_first(k, n):
    half = lax.div(k + 1, 2)
    return jnp.where(lax.rem(k, 2) == 1, n // 2 + half, n // 2 - half)


def iota(shape, dim):
    return lax.broadcasted_iota(jnp.int32, shape, dim)


def kernel(
    res_hbm,
    ck_hbm,
    cv_hbm,
    lens_hbm,
    wq_hbm,
    wk_hbm,
    wv_hbm,
    wo_hbm,
    hgain_hbm,
    lam_hbm,
    again_hbm,
    mgain_hbm,
    ridt_hbm,
    logitst_hbm,
    gate_hbm,
    up_hbm,
    down_hbm,
    out_ref,
    res_ref,
    lens_ref,
    wq_ref,
    wk_ref,
    wv_ref,
    wo_ref,
    hgain_ref,
    lam_ref,
    again_ref,
    mgain_ref,
    ridt_ref,
    logitst_ref,
    kbuf,
    vbuf,
    gbuf,
    ubuf,
    dbuf,
    loc_sem,
    wkv,
    wzq,
    wzk,
    woz,
    woy,
    woa,
    sqs,
    sqr,
    nall,
    mgs,
    mga,
    sb,
    rb,
    ebuf,
    cosb,
    sinb,
    kvs,
    kvr,
    kvo,
    hb,
    hr,
    lhs,
    gz_s,
    gz_r,
    gown,
    gall,
    ds,
    dr,
    xb,
    fs,
    fr,
    zs,
    zr,
    s_wzq,
    r_wzq,
    s_wzk,
    r_wzk,
    s_wo,
    r_wo,
    s_wo2,
    r_wo2,
    s_woa,
    r_woa,
    s_sq,
    r_sq,
    s_na,
    r_na,
    s_mg,
    r_mg,
    s_rb,
    r_rb,
    s_kv,
    r_kv,
    s_h,
    r_h,
    s_woc,
    r_woc,
    s_woy,
    r_woy,
    s_gz,
    r_gz,
    s_ga,
    r_ga,
    s_d,
    r_d,
    s_x,
    r_x,
    s_ew,
    r_ew,
    s_f,
    r_f,
    s_z,
    r_z,
):
    z = lax.axis_index("ep_0")
    x = lax.axis_index("ep_1")
    c = lax.axis_index("ep_2")
    y = lax.axis_index("tp")
    g = x * NC + c
    p = g * NY + y
    twin = x * NC + 1 - c
    q16 = x * NY + y

    def plane_id(other):
        og = lax.div(other, NY)
        return {"ep_1": lax.div(og, NC), "ep_2": lax.rem(og, NC), "tp": lax.rem(other, NY)}

    def along_z(k):
        dest = lax.rem(z + far_first(k, NZ), NZ)
        return dest, {"ep_0": dest, "ep_2": 1 - c}

    def in_plane(k):
        ox = lax.rem(x + far_first(lax.div(k, NY), NX), NX)
        oy = lax.rem(y + far_first(lax.rem(k, NY), NY), NY)
        return ox, oy

    def to(src, dst, ssem, rsem, dev):
        pltpu.make_async_remote_copy(
            src_ref=src, dst_ref=dst, send_sem=ssem, recv_sem=rsem, device_id=dev, device_id_type=MESH
        ).start()

    def drain(ref, sem):
        pltpu.make_async_copy(ref, ref, sem).wait()

    barrier = pltpu.get_barrier_semaphore()

    @pl.loop(0, NZ - 1, unroll=True)
    def _(k):
        pl.semaphore_signal(barrier, inc=1, device_id=along_z(k)[1], device_id_type=MESH)

    for step in (1, 14, 15):
        pl.semaphore_signal(
            barrier, inc=1, device_id={"ep_0": lax.rem(z + step, NZ)}, device_id_type=MESH
        )

    @pl.loop(1, NP, unroll=True)
    def _(k):
        pl.semaphore_signal(
            barrier, inc=1, device_id=plane_id(lax.rem(p + k, NP)), device_id_type=MESH
        )

    small = [
        pltpu.make_async_copy(src, dst, loc_sem.at[k])
        for k, (src, dst) in enumerate(
            (
                (res_hbm, res_ref),
                (wq_hbm, wq_ref),
                (wk_hbm, wk_ref),
                (wv_hbm, wv_ref),
                (wo_hbm, wo_ref),
                (mgain_hbm, mgain_ref),
                (again_hbm, again_ref),
                (hgain_hbm, hgain_ref),
                (ridt_hbm, ridt_ref),
                (logitst_hbm, logitst_ref),
                (lens_hbm, lens_ref),
                (lam_hbm, lam_ref),
            )
        )
    ]
    experts = [
        pltpu.make_async_copy(gate_hbm.at[0], gbuf.at[c], loc_sem.at[12]),
        pltpu.make_async_copy(up_hbm.at[0], ubuf.at[c], loc_sem.at[13]),
        pltpu.make_async_copy(down_hbm.at[0], dbuf.at[c], loc_sem.at[14]),
    ]
    caches = [
        pltpu.make_async_copy(ck_hbm, kbuf, loc_sem.at[15]),
        pltpu.make_async_copy(cv_hbm, vbuf, loc_sem.at[16]),
    ]
    for copy in small + experts + caches:
        copy.start()
    for copy in small:
        copy.wait()
    wkv[...] = jnp.concatenate([wk_ref[...].astype(F32), wv_ref[...].astype(F32)], axis=0).astype(BF)
    stream = res_ref[...].astype(F32)
    own_squares = jnp.broadcast_to(jnp.sum(stream * stream, axis=1, keepdims=True), (16, 128))
    sqs[...] = own_squares
    mgs[...] = jnp.broadcast_to(mgain_ref[...].astype(F32).reshape(1, 256), (8, 256))

    groups = lax.shift_right_logical(ridt_ref[0:1, :], 3).astype(F32)
    grow = jnp.broadcast_to(groups, (16, 16))
    eye = (iota((16, 16), 0) == iota((16, 16), 1)).astype(F32)
    gcol = nt(eye, grow)
    before = jnp.logical_and(grow == gcol, iota((16, 16), 0) < iota((16, 16), 1))
    rank = jnp.sum(jnp.where(before, 1.0, 0.0), axis=0, keepdims=True)
    slot = groups * SLOTS + rank
    dispatch = jnp.where(iota((32, 16), 0).astype(F32) == slot, 1.0, 0.0)
    combine = nt(eye, dispatch)
    logits = logitst_ref[...]
    exps = jnp.exp(logits - jnp.max(logits, axis=0, keepdims=True))
    gates = exps / jnp.sum(exps, axis=0, keepdims=True)
    members = jnp.zeros((128, 16), F32)
    for k in range(CHOSEN):
        member = jnp.bitwise_and(ridt_ref[k : k + 1, :], GROUP_SIZE - 1)
        members = members + jnp.where(iota((128, 16), 0) == member, gates[k : k + 1, :], 0.0)
    slot_gates = lax.dot_general(
        dispatch, members, (((1,), (1,)), ((), ())), precision=lax.Precision.HIGHEST,
        preferred_element_type=F32,
    )
    for k in range(NZ):
        gz_s[k] = slot_gates[2 * k : 2 * k + 2]

    row = iota((1024, 256), 0)
    col = iota((1024, 256), 1)
    src_g = jnp.bitwise_xor(lax.shift_right_logical(row, 7), 1)
    src_lane = jnp.bitwise_and(row, 127)
    to_query = jnp.bitwise_and(col, 63) == src_g * 8 + jnp.bitwise_and(src_lane, 7)
    ebuf[:, 0:256] = jnp.where(to_query, 1.0, 0.0).astype(BF)
    src_r = jnp.bitwise_and(src_lane, 3)
    spot = lax.shift_right_logical(src_lane, 2) * 16 + src_g * 2 + jnp.bitwise_and(src_r, 1)
    on_spot = jnp.logical_and(col == spot, src_lane < 64)
    ebuf[:, 256:512] = jnp.where(jnp.logical_and(on_spot, src_r < 2), 1.0, 0.0).astype(BF)
    ebuf[:, 512:768] = jnp.where(jnp.logical_and(on_spot, src_r >= 2), 1.0, 0.0).astype(BF)

    lane = iota((8, 128), 1)
    sub = iota((8, 128), 0)
    place = jnp.zeros((8, 128), F32)
    for s in range(OWN):
        place = jnp.where(
            jnp.bitwise_and(sub, 3) == s, lens_ref[y * OWN + s].astype(F32), place
        )
    for k in range(NG):
        at_query = ((k ^ 1) % (NG // 2)) * 8 + jnp.bitwise_and(lane, 7)
        at_key = (
            jnp.bitwise_and(lax.shift_right_logical(lane, 2), 1) * 16
            + (k ^ 1) * 2
            + jnp.bitwise_and(lane, 1)
        )
        entry = jnp.where(sub < 4, at_query, at_key).astype(F32)
        angle = place * jnp.exp(entry * (-math.log(rotary_base) / (HEAD_DIM // 2)))
        cosb[k] = jnp.cos(angle)
        sinb[k] = jnp.sin(angle)

    pl.semaphore_wait(barrier, NZ - 1 + NP - 1 + 3)

    @pl.loop(1, NY, unroll=True)
    def _(k):
        dev = {"tp": lax.rem(y + k, NY)}
        to(sqs, sqr.at[y], s_sq, r_sq, dev)
        to(mgs, mga.at[y], s_mg, r_mg, dev)

    z_low, z_high = lax.rem(z, 4), lax.div(z, 4)
    for step in (8, 4, 12, 0):
        dev = {"ep_0": lax.rem(z + step, NZ), "ep_2": 1 - c}
        to(wo_ref, woz.at[z_low, z_high], s_wo, r_wo, dev)

    @pl.loop(0, NZ, unroll=True)
    def _(k):
        dev = along_z(k)[1]
        to(wq_ref, wzq.at[z], s_wzq, r_wzq, dev)
        to(wkv, wzk.at[z], s_wzk, r_wzk, dev)

    sqr[y] = own_squares
    mga[y] = mgs[...]
    drain(sqr.at[pl.ds(0, NY - 1)], r_sq)
    squares = sqr[0] + sqr[1] + sqr[2] + sqr[3]
    scale = lax.rsqrt(squares[:, 0:1] / WIDTH + norm_eps)
    normed = (stream * scale * again_ref[...].astype(F32).reshape(1, 256)).astype(BF)
    nall[g] = normed

    @pl.loop(1, NG, unroll=True)
    def _(k):
        other = lax.rem(g + k, NG)
        to(
            nall.at[g], nall.at[g], s_na, r_na,
            {"ep_1": lax.div(other, NC), "ep_2": lax.rem(other, NC)},
        )

    @pl.loop(0, NZ, unroll=True)
    def _(k):
        dest, dev = along_z(k)
        to(gz_s.at[dest], gz_r.at[k], s_gz, r_gz, dev)

    partner = {"ep_2": 1 - c}
    for copy in experts:
        copy.wait()
    for k, ref in enumerate((gbuf, ubuf, dbuf)):
        to(ref.at[c], ref.at[c], s_ew.at[k], r_ew.at[k], partner)

    drain(nall.at[pl.ds(0, NG - 1)], r_na)
    drain(woz.at[0], r_wo)
    for step in (2, 1, 15):
        to(woz.at[z_low], woz.at[z_low], s_wo2, r_wo2, {"ep_0": lax.rem(z + step, NZ)})

    drain(wzq, r_wzq)
    drain(wzk, r_wzk)
    tokens = nall[...].reshape(128, 256)
    part_q = nt(tokens, wzq[...].reshape(128, 256))
    part_kv = nt(tokens, wzk[...].reshape(64, 256))
    part_kv = jnp.concatenate([part_kv, jnp.zeros((128, 64), F32)], axis=1)
    for k in range(NP):
        sb[k, 0:4, :] = part_q[4 * k : 4 * k + 4]
        sb[k, 4:8, :] = part_kv[4 * k : 4 * k + 4]

    @pl.loop(0, NX * NY, unroll=True)
    def _(k):
        ox, oy = in_plane(k)
        other = (ox * NC + 1 - c) * NY + oy
        to(sb.at[other], rb.at[p], s_rb, r_rb, plane_id(other))

        @pl.when(k < NX * NY - 1)
        def _():
            same = (ox * NC + c) * NY + oy
            to(sb.at[same], rb.at[p], s_rb, r_rb, plane_id(same))

    rb[p] = sb[p]

    drain(woz.at[pl.ds(0, 3)], r_wo2)
    woy[y] = woz[:, y]

    @pl.loop(1, NY, unroll=True)
    def _(k):
        other = lax.rem(y + k, NY)
        to(woz.at[:, other], woy.at[y], s_woy, r_woy, {"tp": other})

    drain(gz_r, r_gz)
    for k in range(NZ):
        gown[2 * k : 2 * k + 2, :] = gz_r[k]
    gall[x] = gown[...]

    @pl.loop(1, NX, unroll=True)
    def _(k):
        to(gown, gall.at[x], s_ga, r_ga, {"ep_1": lax.rem(x + k, NX)})

    drain(rb.at[pl.ds(0, NP - 1)], r_rb)
    parts = rb[...].reshape(NG, NY, 8, 128)
    raw = parts[:, 0] + parts[:, 1] + parts[:, 2] + parts[:, 3]
    is_query = sub < 4
    is_key = jnp.logical_and(lane < 64, jnp.bitwise_and(lane, 3) < 2)
    low_key = jnp.bitwise_and(lane, 15) < 8
    turned = []
    for k in range(NG):
        own = raw[k]
        pair = raw[(k + NG // 2) % NG]
        if k < NG // 2:
            pair = -pair
        above = pltpu.roll(own, 120, 1)
        below = pltpu.roll(own, 8, 1)
        key_pair = jnp.where(low_key, -above, below)
        spun = own * cosb[k] + jnp.where(is_query, pair, key_pair) * sinb[k]
        turned.append(jnp.where(jnp.logical_or(is_query, is_key), spun, own))
    rows8 = jnp.concatenate([t.astype(BF) for t in turned], axis=1)
    placed = nn(rows8, ebuf[:, 256:768])
    kvs[...] = placed
    kvr[y] = placed

    @pl.loop(1, NY, unroll=True)
    def _(k):
        to(kvs, kvr.at[y], s_kv, r_kv, {"tp": lax.rem(y + k, NY)})

    own_keys = placed[4:8, 0:256]
    own_values = placed[4:8, 256:512]

    pieces = []
    for s in range(OWN):
        for m in range(2):
            keep = lax.shift_right_logical(lane, 3) == 2 * sub + m
            line = []
            for k in range(NG):
                whole = jnp.broadcast_to(turned[k][s : s + 1, :], (8, 128))
                line.append(jnp.where(keep, whole, 0.0))
            pieces.append(jnp.concatenate(line, axis=1))
    spread = nn(jnp.concatenate(pieces, axis=0).astype(BF), ebuf[:, 0:256])
    drain(woy.at[pl.ds(0, NY - 1)], r_woy)
    woa[:, :, twin] = woy[...]
    to(woy, woa.at[:, :, twin], s_woc, r_woc, partner)

    for k in (2, 1, 3):
        dev = {"ep_1": lax.rem(x + k, NX), "ep_2": 1 - c}
        to(woy, woa.at[:, :, twin], s_woa, r_woa.at[k - 1], dev)

    for copy in caches:
        copy.wait()
    blk = lax.shift_right_logical(iota((16, 256), 1), 6)
    row16 = iota((16, 256), 0)
    own_block = (
        lax.shift_right_logical(jnp.bitwise_and(row16, 7), 2) * 2 + lax.shift_right_logical(row16, 3)
    )
    head_low = jnp.bitwise_and(iota((16, 128), 0), 7) < 4
    lam = jnp.zeros((8, 128), F32)
    for h in range(HEADS):
        lam = jnp.where(sub == h, lam_ref[h], lam)
    for s in range(OWN):
        queries = jnp.where(blk == own_block, spread[16 * s : 16 * s + 16], 0.0)
        scores = nt(queries.astype(BF), kbuf[s]) * 0.125
        length = lens_ref[y * OWN + s]
        scores = jnp.where(iota((16, CACHE), 1) < length, scores, masked_score)
        fresh = jnp.sum(queries * own_keys[s : s + 1], axis=1, keepdims=True) * 0.125
        top = jnp.maximum(jnp.max(scores, axis=1, keepdims=True), fresh)
        weights = jnp.exp(scores - top).astype(BF)
        fresh_weight = jnp.exp(fresh - top).astype(BF).astype(F32)
        total = jnp.sum(weights.astype(F32), axis=1, keepdims=True) + fresh_weight
        mixed = nn(weights, vbuf[s])
        values = jnp.where(
            head_low,
            mixed[:, 0:128] + fresh_weight * own_values[s : s + 1, 0:128],
            mixed[:, 128:256] + fresh_weight * own_values[s : s + 1, 128:256],
        )
        averaged = values / total
        contrast = averaged[0:8] - lam * averaged[8:16]
        contrast = (
            contrast
            * lax.rsqrt(jnp.mean(contrast * contrast, axis=1, keepdims=True) + head_eps)
            * hgain_ref[...].reshape(1, 128)
        )
        rounded = contrast.astype(BF).astype(F32)
        for h in range(HEADS):
            hb[s : s + 1, 128 * h : 128 * h + 128] = rounded[h : h + 1, :]

    hr[y] = hb[...]

    @pl.loop(1, NY, unroll=True)
    def _(k):
        to(hb, hr.at[y], s_h, r_h, {"tp": lax.rem(y + k, NY)})

    for k in (1, 3, 2):
        block = woa.at[:, :, lax.rem(x + NX - k, NX) * NC + c]
        drain(block, r_woa.at[k - 1])
        to(block, block, s_woc, r_woc, partner)

    drain(hr.at[pl.ds(0, NY - 1)], r_h)
    drain(woa.at[:, :, pl.ds(0, NX)], r_woc)
    lined = hr[...].reshape(16, WIDTH).astype(BF)
    attended = jnp.zeros((16, 256), F32)
    for k in range(NY):
        attended = attended + nt(lined[:, 256 * k : 256 * k + 256], woa[k].reshape(256, 256))
    middle = (stream + attended).astype(BF)

    routed = nn(dispatch.astype(BF), middle)
    for k in range(NZ):
        ds[k] = routed[2 * k : 2 * k + 2].astype(ds.dtype)

    @pl.loop(0, NZ, unroll=True)
    def _(k):
        dest, dev = along_z(k)
        to(ds.at[dest], dr.at[k], s_d, r_d.at[lax.div(k, 8)], dev)

    rows = NX * 16

    def spread(b):
        drain(dr.at[pl.ds(8 * b, 8)], r_d.at[b])
        for k in range(8):
            lhs[2 * k : 2 * k + 2, :] = dr[8 * b + k].astype(F32)
        xb[b, x, y] = lhs[0:16].astype(BF)

        @pl.loop(0, NX * NY - 1, unroll=True)
        def _(k):
            ox, oy = in_plane(k)
            to(xb.at[b, x, y], xb.at[b, x, y], s_x.at[b], r_x.at[b], {"ep_1": ox, "tp": oy})

    def run_experts(b):
        wide = [xb[b, :, k].reshape(rows, 256).astype(F32) for k in range(NY)]
        total_sq = jnp.zeros((rows, 1), F32)
        for k in range(NY):
            total_sq = total_sq + jnp.sum(wide[k] * wide[k], axis=1, keepdims=True)
        scale = lax.rsqrt(total_sq / WIDTH + norm_eps)
        mixed_in = [(wide[k] * scale * mga[k, 0:1, :]).astype(BF) for k in range(NY)]
        member = gall[:, 16 * b : 16 * b + 16, :].reshape(rows, 128)
        produced = jnp.zeros((rows, WIDTH), F32)
        for e in range(NC):
            gate_act = jnp.zeros((rows, 128), F32)
            up_act = jnp.zeros((rows, 128), F32)
            for k in range(NY):
                gate_act = gate_act + nn(mixed_in[k], gbuf[e, 256 * k : 256 * k + 256, :])
                up_act = up_act + nn(mixed_in[k], ubuf[e, 256 * k : 256 * k + 256, :])
            hidden = (gate_act / (1.0 + jnp.exp(-gate_act)) * up_act).astype(BF)
            slot_gate = jnp.sum(
                jnp.where(iota((rows, 128), 1) == x * NC + e, member, 0.0), axis=1, keepdims=True
            )
            produced = produced + nn(hidden, dbuf[e]) * slot_gate
        for k in range(NX):
            for j in range(NY):
                fs[b, k, j] = produced[16 * k : 16 * k + 16, 256 * j : 256 * j + 256].astype(BF)

        @pl.loop(0, NX * NY - 1, unroll=True)
        def _(k):
            ox, oy = in_plane(k)
            to(fs.at[b, ox, oy], fr.at[b, q16], s_f.at[b], r_f.at[b], {"ep_1": ox, "tp": oy})

        fr[b, q16] = fs[b, x, y]

    def give_back(b):
        drain(fr.at[b, pl.ds(0, NX * NY - 1)], r_f.at[b])
        mixture = fr[b, 0].astype(F32)
        for k in range(1, NX * NY):
            mixture = mixture + fr[b, k].astype(F32)
        for k in range(8):
            zs[8 * b + k] = mixture[2 * k : 2 * k + 2].astype(zs.dtype)

        @pl.loop(8 * b, 8 * b + 8, unroll=True)
        def _(k):
            source = lax.rem(z + 2 * NZ - far_first(k, NZ), NZ)
            to(zs.at[k], zr.at[z], s_z, r_z, {"ep_0": source, "ep_2": 1 - c})

    spread(1)
    spread(0)
    drain(gall.at[pl.ds(0, NX - 1)], r_ga)
    drain(mga.at[pl.ds(0, NY - 1)], r_mg)
    for k, ref in enumerate((gbuf, ubuf, dbuf)):
        drain(ref.at[0], r_ew.at[k])
    drain(fr.at[1, pl.ds(0, NX * NY - 1)], r_x.at[1])
    run_experts(1)
    drain(fr.at[0, pl.ds(0, NX * NY - 1)], r_x.at[0])
    run_experts(0)
    give_back(1)
    give_back(0)

    drain(kvr.at[pl.ds(0, NY - 1)], r_kv)
    for k in range(NY):
        kvo[4 * k : 4 * k + 4, :] = kvr[k, 4:8, :]
    out_ref[1] = kvo[:, 0:256].astype(BF)
    out_ref[2] = kvo[:, 256:512].astype(BF)

    drain(zr, r_z)
    for k in range(NZ):
        lhs[2 * k : 2 * k + 2, :] = zr[k].astype(F32)
    mix = nn(combine.astype(BF), lhs[...].astype(BF))
    out_ref[0] = (middle.astype(F32) + mix).astype(BF)

    for ref, sem in (
        (wzq, s_wzq),
        (wzk, s_wzk),
        (woz.at[0], s_wo),
        (woz.at[pl.ds(0, 3)], s_wo2),
        (gz_r, s_gz),
        (dr, s_d),
        (zr, s_z),
    ):
        drain(ref, sem)
    for ref, sem in ((sqr, s_sq), (mga, s_mg), (kvr, s_kv), (hr, s_h), (woy, s_woy)):
        drain(ref.at[pl.ds(0, NY - 1)], sem)
    drain(nall.at[pl.ds(0, NG - 1)], s_na)
    drain(gall.at[pl.ds(0, NX - 1)], s_ga)
    for k, ref in enumerate((gbuf, ubuf, dbuf)):
        drain(ref.at[0], s_ew.at[k])
    drain(woa.at[:, :, pl.ds(0, NX - 1)], s_woa)
    drain(woa.at[:, :, pl.ds(0, NX)], s_woc)
    drain(rb.at[pl.ds(0, NP - 1)], s_rb)
    for b in range(2):
        drain(fr.at[b, pl.ds(0, NX * NY - 1)], s_x.at[b])
        drain(fr.at[b, pl.ds(0, NX * NY - 1)], s_f.at[b])


def on_device(
    residual,
    cache_keys,
    cache_values,
    lengths,
    query_weight,
    key_weight,
    value_weight,
    out_weight,
    head_gain,
    mix_lambda,
    attn_gain,
    moe_gain,
    route_ids,
    route_logits,
    gate_weight,
    up_weight,
    down_weight,
):
    vm = pl.BlockSpec(memory_space=pltpu.VMEM)
    hbm = pl.BlockSpec(memory_space=pl.ANY)
    dma = pltpu.SemaphoreType.DMA
    V = pltpu.VMEM
    scratch = [
        V((16, 256), BF),
        pltpu.SMEM((16,), jnp.int32),
        V((8, 256), BF),
        V((2, 256), BF),
        V((2, 256), BF),
        V((8, 256), BF),
        V((128,), F32),
        pltpu.SMEM((HEADS,), F32),
        V((256,), BF),
        V((256,), BF),
        V((CHOSEN, 16), jnp.int32),
        V((CHOSEN, 16), F32),
        V((OWN, CACHE, 256), BF),
        V((OWN, CACHE, 256), BF),
        V((NC, WIDTH, 128), BF),
        V((NC, WIDTH, 128), BF),
        V((NC, 128, WIDTH), BF),
        dma((17,)),
        V((4, 256), BF),
        V((NZ, 8, 256), BF),
        V((NZ, 4, 256), BF),
        V((4, NZ // 4, 8, 256), BF),
        V((NY, NZ // NY, 8, 256), BF),
        V((NY, NZ // NY, NG, 8, 256), BF),
        V((16, 128), F32),
        V((NY, 16, 128), F32),
        V((NG, 16, 256), BF),
        V((8, 256), F32),
        V((NY, 8, 256), F32),
        V((NP, 8, 128), F32),
        V((NP, 8, 128), F32),
        V((1024, 768), BF),
        V((NG, 8, 128), F32),
        V((NG, 8, 128), F32),
        V((8, 512), F32),
        V((NY, 8, 512), F32),
        V((16, 512), F32),
        V((OWN, WIDTH), F32),
        V((NY, OWN, WIDTH), F32),
        V((32, 256), F32),
        V((NZ, SLOTS, 128), F32),
        V((NZ, SLOTS, 128), F32),
        V((32, 128), F32),
        V((NX, 32, 128), F32),
        V((NZ, SLOTS, 256), BF),
        V((NZ, SLOTS, 256), BF),
        V((2, NX, NY, 16, 256), BF),
        V((2, NX, NY, 16, 256), BF),
        V((2, NX * NY, 16, 256), BF),
        V((NZ, SLOTS, 256), BF),
        V((NZ, SLOTS, 256), BF),
    ]
    sems = [dma] * 40
    for k in (31, 32, 33, 36, 37):
        sems[k] = dma((2,))
    sems[34] = sems[35] = dma((3,))
    sems[9] = dma((3,))
    results = pl.pallas_call(
        kernel,
        out_shape=pltpu.VMEM((3, 16, 256), BF),
        in_specs=[hbm] * 17,
        out_specs=vm,
        scratch_shapes=scratch + sems,
        compiler_params=pltpu.CompilerParams(collective_id=0, has_side_effects=True),
        cost_estimate=pl.CostEstimate(flops=10**9, bytes_accessed=5 * 10**6, transcendentals=0),
    )(
        residual,
        cache_keys,
        cache_values,
        lengths,
        query_weight.T,
        key_weight.T,
        value_weight.T,
        out_weight.T,
        head_gain,
        mix_lambda,
        attn_gain,
        moe_gain,
        route_ids.T,
        route_logits.T,
        gate_weight,
        up_weight,
        down_weight,
    )
    return results[0], results[1], results[2]


def solution(mesh):
    torus = Mesh(mesh.devices.reshape(NZ, NX, NC, NY), ("ep_0", "ep_1", "ep_2", "tp"))
    return jax.shard_map(
        on_device,
        mesh=torus,
        in_specs=(
            P(EP, "tp"),
            P(EP_TP, None, None),
            P(EP_TP, None, None),
            P(EP),
            P("tp", EP),
            P("tp", EP),
            P("tp", EP),
            P("tp", EP),
            P(),
            P(),
            P("tp"),
            P("tp"),
            P(EP, None),
            P(EP, None),
            P(EP, None, "tp"),
            P(EP, None, "tp"),
            P(EP, "tp", None),
        ),
        out_specs=(P(EP, "tp"), P(EP, None), P(EP, None)),
        check_vma=False,
    )
```

```python
import math

import jax
import jax.numpy as jnp
from jax import lax
from jax.experimental import pallas as pl
from jax.experimental.pallas import tpu as pltpu
from jax.sharding import Mesh
from jax.sharding import PartitionSpec as P

WIDTH = 1024
HEADS = 8
HEAD_DIM = 64
VALUE_DIM = 128
CHOSEN = 6
GROUP_SIZE = 8
SLOTS = 2
EP = ("ep_0", "ep_1", "ep_2")
EP_TP = ("ep_0", "ep_1", "ep_2", "tp")
NZ, NX, NC, NY = 16, 4, 2, 4
NG = NX * NC
NP = NG * NY
CACHE = 1024
OWN = 4

norm_eps = 1e-06
head_eps = 1e-05
masked_score = -1e30
rotary_base = 500000.0

MESH = pl.DeviceIdType.MESH
BF = jnp.bfloat16
F32 = jnp.float32


def nt(a, b):
    return lax.dot_general(a, b, (((1,), (1,)), ((), ())), preferred_element_type=F32)


def nn(a, b):
    return lax.dot_general(a, b, (((1,), (0,)), ((), ())), preferred_element_type=F32)


def far_first(k, n):
    half = lax.div(k + 1, 2)
    return jnp.where(lax.rem(k, 2) == 1, n // 2 + half, n // 2 - half)


def iota(shape, dim):
    return lax.broadcasted_iota(jnp.int32, shape, dim)


def kernel(
    res_hbm,
    ck_hbm,
    cv_hbm,
    lens_hbm,
    wq_hbm,
    wk_hbm,
    wv_hbm,
    wo_hbm,
    hgain_hbm,
    lam_hbm,
    again_hbm,
    mgain_hbm,
    ridt_hbm,
    logitst_hbm,
    gate_hbm,
    up_hbm,
    down_hbm,
    out_ref,
    res_ref,
    lens_ref,
    wq_ref,
    wk_ref,
    wv_ref,
    wo_ref,
    hgain_ref,
    lam_ref,
    again_ref,
    mgain_ref,
    ridt_ref,
    logitst_ref,
    kbuf,
    vbuf,
    gbuf,
    ubuf,
    dbuf,
    loc_sem,
    wkv,
    wzq,
    wzk,
    woz,
    woy,
    woa,
    sqs,
    sqr,
    nall,
    mgs,
    mga,
    sb,
    rb,
    ebuf,
    cosb,
    sinb,
    kvs,
    kvr,
    kvo,
    hb,
    hr,
    lhs,
    gz_s,
    gz_r,
    gown,
    gall,
    ds,
    dr,
    xb,
    fs,
    fr,
    zs,
    zr,
    s_wzq,
    r_wzq,
    s_wzk,
    r_wzk,
    s_wo,
    r_wo,
    s_wo2,
    r_wo2,
    s_woa,
    r_woa,
    s_sq,
    r_sq,
    s_na,
    r_na,
    s_mg,
    r_mg,
    s_rb,
    r_rb,
    s_kv,
    r_kv,
    s_h,
    r_h,
    s_woc,
    r_woc,
    s_woy,
    r_woy,
    s_gz,
    r_gz,
    s_ga,
    r_ga,
    s_d,
    r_d,
    s_x,
    r_x,
    s_ew,
    r_ew,
    s_f,
    r_f,
    s_z,
    r_z,
):
    z = lax.axis_index("ep_0")
    x = lax.axis_index("ep_1")
    c = lax.axis_index("ep_2")
    y = lax.axis_index("tp")
    g = x * NC + c
    p = g * NY + y
    twin = x * NC + 1 - c
    q16 = x * NY + y

    def plane_id(other):
        og = lax.div(other, NY)
        return {"ep_1": lax.div(og, NC), "ep_2": lax.rem(og, NC), "tp": lax.rem(other, NY)}

    def along_z(k):
        dest = lax.rem(z + far_first(k, NZ), NZ)
        return dest, {"ep_0": dest, "ep_2": 1 - c}

    def in_plane(k):
        ox = lax.rem(x + far_first(lax.div(k, NY), NX), NX)
        oy = lax.rem(y + far_first(lax.rem(k, NY), NY), NY)
        return ox, oy

    def to(src, dst, ssem, rsem, dev):
        pltpu.make_async_remote_copy(
            src_ref=src, dst_ref=dst, send_sem=ssem, recv_sem=rsem, device_id=dev, device_id_type=MESH
        ).start()

    def drain(ref, sem):
        pltpu.make_async_copy(ref, ref, sem).wait()

    barrier = pltpu.get_barrier_semaphore()

    @pl.loop(0, NZ - 1, unroll=True)
    def _(k):
        pl.semaphore_signal(barrier, inc=1, device_id=along_z(k)[1], device_id_type=MESH)

    for step in (1, 14, 15):
        pl.semaphore_signal(
            barrier, inc=1, device_id={"ep_0": lax.rem(z + step, NZ)}, device_id_type=MESH
        )

    @pl.loop(1, NP, unroll=True)
    def _(k):
        pl.semaphore_signal(
            barrier, inc=1, device_id=plane_id(lax.rem(p + k, NP)), device_id_type=MESH
        )

    small = [
        pltpu.make_async_copy(src, dst, loc_sem.at[k])
        for k, (src, dst) in enumerate(
            (
                (res_hbm, res_ref),
                (wq_hbm, wq_ref),
                (wk_hbm, wk_ref),
                (wv_hbm, wv_ref),
                (wo_hbm, wo_ref),
                (mgain_hbm, mgain_ref),
                (again_hbm, again_ref),
                (hgain_hbm, hgain_ref),
                (ridt_hbm, ridt_ref),
                (logitst_hbm, logitst_ref),
                (lens_hbm, lens_ref),
                (lam_hbm, lam_ref),
            )
        )
    ]
    experts = [
        pltpu.make_async_copy(gate_hbm.at[0], gbuf.at[c], loc_sem.at[12]),
        pltpu.make_async_copy(up_hbm.at[0], ubuf.at[c], loc_sem.at[13]),
        pltpu.make_async_copy(down_hbm.at[0], dbuf.at[c], loc_sem.at[14]),
    ]
    caches = [
        pltpu.make_async_copy(ck_hbm, kbuf, loc_sem.at[15]),
        pltpu.make_async_copy(cv_hbm, vbuf, loc_sem.at[16]),
    ]
    for copy in small + experts + caches:
        copy.start()
    for copy in small:
        copy.wait()
    wkv[...] = jnp.concatenate([wk_ref[...].astype(F32), wv_ref[...].astype(F32)], axis=0).astype(BF)
    stream = res_ref[...].astype(F32)
    own_squares = jnp.broadcast_to(jnp.sum(stream * stream, axis=1, keepdims=True), (16, 128))
    sqs[...] = own_squares
    mgs[...] = jnp.broadcast_to(mgain_ref[...].astype(F32).reshape(1, 256), (8, 256))

    groups = lax.shift_right_logical(ridt_ref[0:1, :], 3).astype(F32)
    grow = jnp.broadcast_to(groups, (16, 16))
    eye = (iota((16, 16), 0) == iota((16, 16), 1)).astype(F32)
    gcol = nt(eye, grow)
    before = jnp.logical_and(grow == gcol, iota((16, 16), 0) < iota((16, 16), 1))
    rank = jnp.sum(jnp.where(before, 1.0, 0.0), axis=0, keepdims=True)
    slot = groups * SLOTS + rank
    dispatch = jnp.where(iota((32, 16), 0).astype(F32) == slot, 1.0, 0.0)
    combine = nt(eye, dispatch)
    logits = logitst_ref[...]
    exps = jnp.exp(logits - jnp.max(logits, axis=0, keepdims=True))
    gates = exps / jnp.sum(exps, axis=0, keepdims=True)
    members = jnp.zeros((128, 16), F32)
    for k in range(CHOSEN):
        member = jnp.bitwise_and(ridt_ref[k : k + 1, :], GROUP_SIZE - 1)
        members = members + jnp.where(iota((128, 16), 0) == member, gates[k : k + 1, :], 0.0)
    slot_gates = lax.dot_general(
        dispatch, members, (((1,), (1,)), ((), ())), precision=lax.Precision.HIGHEST,
        preferred_element_type=F32,
    )
    for k in range(NZ):
        gz_s[k] = slot_gates[2 * k : 2 * k + 2]

    row = iota((1024, 256), 0)
    col = iota((1024, 256), 1)
    src_g = jnp.bitwise_xor(lax.shift_right_logical(row, 7), 1)
    src_lane = jnp.bitwise_and(row, 127)
    to_query = jnp.bitwise_and(col, 63) == src_g * 8 + jnp.bitwise_and(src_lane, 7)
    ebuf[:, 0:256] = jnp.where(to_query, 1.0, 0.0).astype(BF)
    src_r = jnp.bitwise_and(src_lane, 3)
    spot = lax.shift_right_logical(src_lane, 2) * 16 + src_g * 2 + jnp.bitwise_and(src_r, 1)
    on_spot = jnp.logical_and(col == spot, src_lane < 64)
    ebuf[:, 256:512] = jnp.where(jnp.logical_and(on_spot, src_r < 2), 1.0, 0.0).astype(BF)
    ebuf[:, 512:768] = jnp.where(jnp.logical_and(on_spot, src_r >= 2), 1.0, 0.0).astype(BF)

    lane = iota((8, 128), 1)
    sub = iota((8, 128), 0)
    place = jnp.zeros((8, 128), F32)
    for s in range(OWN):
        place = jnp.where(
            jnp.bitwise_and(sub, 3) == s, lens_ref[y * OWN + s].astype(F32), place
        )
    for k in range(NG):
        at_query = ((k ^ 1) % (NG // 2)) * 8 + jnp.bitwise_and(lane, 7)
        at_key = (
            jnp.bitwise_and(lax.shift_right_logical(lane, 2), 1) * 16
            + (k ^ 1) * 2
            + jnp.bitwise_and(lane, 1)
        )
        entry = jnp.where(sub < 4, at_query, at_key).astype(F32)
        angle = place * jnp.exp(entry * (-math.log(rotary_base) / (HEAD_DIM // 2)))
        cosb[k] = jnp.cos(angle)
        sinb[k] = jnp.sin(angle)

    pl.semaphore_wait(barrier, NZ - 1 + NP - 1 + 3)

    @pl.loop(1, NY, unroll=True)
    def _(k):
        dev = {"tp": lax.rem(y + k, NY)}
        to(sqs, sqr.at[y], s_sq, r_sq, dev)
        to(mgs, mga.at[y], s_mg, r_mg, dev)

    z_low, z_high = lax.rem(z, 4), lax.div(z, 4)
    for step in (8, 4, 12, 0):
        dev = {"ep_0": lax.rem(z + step, NZ), "ep_2": 1 - c}
        to(wo_ref, woz.at[z_low, z_high], s_wo, r_wo, dev)

    @pl.loop(0, NZ, unroll=True)
    def _(k):
        dev = along_z(k)[1]
        to(wq_ref, wzq.at[z], s_wzq, r_wzq, dev)
        to(wkv, wzk.at[z], s_wzk, r_wzk, dev)

    sqr[y] = own_squares
    mga[y] = mgs[...]
    drain(sqr.at[pl.ds(0, NY - 1)], r_sq)
    squares = sqr[0] + sqr[1] + sqr[2] + sqr[3]
    scale = lax.rsqrt(squares[:, 0:1] / WIDTH + norm_eps)
    normed = (stream * scale * again_ref[...].astype(F32).reshape(1, 256)).astype(BF)
    nall[g] = normed

    @pl.loop(1, NG, unroll=True)
    def _(k):
        other = lax.rem(g + k, NG)
        to(
            nall.at[g], nall.at[g], s_na, r_na,
            {"ep_1": lax.div(other, NC), "ep_2": lax.rem(other, NC)},
        )

    @pl.loop(0, NZ, unroll=True)
    def _(k):
        dest, dev = along_z(k)
        to(gz_s.at[dest], gz_r.at[k], s_gz, r_gz, dev)

    partner = {"ep_2": 1 - c}
    for copy in experts:
        copy.wait()
    for k, ref in enumerate((gbuf, ubuf, dbuf)):
        to(ref.at[c], ref.at[c], s_ew.at[k], r_ew.at[k], partner)

    drain(nall.at[pl.ds(0, NG - 1)], r_na)
    drain(woz.at[0], r_wo)
    for step in (2, 1, 15):
        to(woz.at[z_low], woz.at[z_low], s_wo2, r_wo2, {"ep_0": lax.rem(z + step, NZ)})

    drain(wzq, r_wzq)
    drain(wzk, r_wzk)
    tokens = nall[...].reshape(128, 256)
    part_q = nt(tokens, wzq[...].reshape(128, 256))
    part_kv = nt(tokens, wzk[...].reshape(64, 256))
    part_kv = jnp.concatenate([part_kv, jnp.zeros((128, 64), F32)], axis=1)
    for k in range(NP):
        sb[k, 0:4, :] = part_q[4 * k : 4 * k + 4]
        sb[k, 4:8, :] = part_kv[4 * k : 4 * k + 4]

    @pl.loop(0, NX * NY, unroll=True)
    def _(k):
        ox, oy = in_plane(k)
        other = (ox * NC + 1 - c) * NY + oy
        to(sb.at[other], rb.at[p], s_rb, r_rb, plane_id(other))

        @pl.when(k < NX * NY - 1)
        def _():
            same = (ox * NC + c) * NY + oy
            to(sb.at[same], rb.at[p], s_rb, r_rb, plane_id(same))

    rb[p] = sb[p]

    drain(woz.at[pl.ds(0, 3)], r_wo2)
    woy[y] = woz[:, y]
    over_x = [(k, {"ep_1": lax.rem(x + k, NX), "ep_2": 1 - c}) for k in (2, 1, 3)]

    @pl.loop(1, NY, unroll=True)
    def _(k):
        other = lax.rem(y + k, NY)
        to(woz.at[:, other], woy.at[y], s_woy, r_woy, {"tp": other})

    for k, dev in over_x:
        to(woz.at[:, y], woa.at[y, :, twin], s_woa, r_woa.at[k - 1], dev)

    drain(woy.at[pl.ds(0, NY - 1)], r_woy)
    woa[:, :, twin] = woy[...]
    to(woy, woa.at[:, :, twin], s_woc, r_woc, partner)

    for k, dev in over_x:
        for j in range(1, NY):
            piece = lax.rem(y + j, NY)
            to(woy.at[piece], woa.at[piece, :, twin], s_woa, r_woa.at[k - 1], dev)

    drain(rb.at[pl.ds(0, NP - 1)], r_rb)
    parts = rb[...].reshape(NG, NY, 8, 128)
    raw = parts[:, 0] + parts[:, 1] + parts[:, 2] + parts[:, 3]
    is_query = sub < 4
    is_key = jnp.logical_and(lane < 64, jnp.bitwise_and(lane, 3) < 2)
    low_key = jnp.bitwise_and(lane, 15) < 8
    turned = []
    for k in range(NG):
        own = raw[k]
        pair = raw[(k + NG // 2) % NG]
        if k < NG // 2:
            pair = -pair
        above = pltpu.roll(own, 120, 1)
        below = pltpu.roll(own, 8, 1)
        key_pair = jnp.where(low_key, -above, below)
        spun = own * cosb[k] + jnp.where(is_query, pair, key_pair) * sinb[k]
        turned.append(jnp.where(jnp.logical_or(is_query, is_key), spun, own))
    rows8 = jnp.concatenate([t.astype(BF) for t in turned], axis=1)
    placed = nn(rows8, ebuf[:, 256:768])
    kvs[...] = placed
    kvr[y] = placed

    own_keys = placed[4:8, 0:256]
    own_values = placed[4:8, 256:512]

    pieces = []
    for s in range(OWN):
        for m in range(2):
            keep = lax.shift_right_logical(lane, 3) == 2 * sub + m
            line = []
            for k in range(NG):
                whole = jnp.broadcast_to(turned[k][s : s + 1, :], (8, 128))
                line.append(jnp.where(keep, whole, 0.0))
            pieces.append(jnp.concatenate(line, axis=1))
    spread = nn(jnp.concatenate(pieces, axis=0).astype(BF), ebuf[:, 0:256])
    for copy in caches:
        copy.wait()
    blk = lax.shift_right_logical(iota((16, 256), 1), 6)
    row16 = iota((16, 256), 0)
    own_block = (
        lax.shift_right_logical(jnp.bitwise_and(row16, 7), 2) * 2 + lax.shift_right_logical(row16, 3)
    )
    head_low = jnp.bitwise_and(iota((16, 128), 0), 7) < 4
    lam = jnp.zeros((8, 128), F32)
    for h in range(HEADS):
        lam = jnp.where(sub == h, lam_ref[h], lam)
    queries = [jnp.where(blk == own_block, spread[16 * s : 16 * s + 16], 0.0) for s in range(OWN)]
    scores = jnp.concatenate([nt(queries[s].astype(BF), kbuf[s]) for s in range(OWN)], axis=0) * 0.125
    fresh = jnp.concatenate(
        [jnp.sum(queries[s] * own_keys[s : s + 1], axis=1, keepdims=True) for s in range(OWN)], axis=0
    ) * 0.125
    seq_of = lax.shift_right_logical(iota((16 * OWN, 1), 0), 4)
    length = jnp.zeros((16 * OWN, 1), jnp.int32)
    for s in range(OWN):
        length = jnp.where(seq_of == s, lens_ref[y * OWN + s], length)
    scores = jnp.where(iota((16 * OWN, CACHE), 1) < length, scores, masked_score)
    top = jnp.maximum(jnp.max(scores, axis=1, keepdims=True), fresh)
    weights = jnp.exp(scores - top).astype(BF)
    fresh_weight = jnp.exp(fresh - top).astype(BF).astype(F32)
    total = jnp.sum(weights.astype(F32), axis=1, keepdims=True) + fresh_weight
    mixed = [nn(weights[16 * s : 16 * s + 16], vbuf[s]) for s in range(OWN)]
    contrasts = []
    for s in range(OWN):
        here = slice(16 * s, 16 * s + 16)
        fresh_here = fresh_weight[here]
        values = jnp.where(
            head_low,
            mixed[s][:, 0:128] + fresh_here * own_values[s : s + 1, 0:128],
            mixed[s][:, 128:256] + fresh_here * own_values[s : s + 1, 128:256],
        )
        averaged = values / total[here]
        contrasts.append(averaged[0:8] - lam * averaged[8:16])
    contrast = jnp.concatenate(contrasts, axis=0)
    contrast = (
        contrast
        * lax.rsqrt(jnp.mean(contrast * contrast, axis=1, keepdims=True) + head_eps)
        * hgain_ref[...].reshape(1, 128)
    )
    rounded = contrast.astype(BF).astype(F32)
    for s in range(OWN):
        for h in range(HEADS):
            at = HEADS * s + h
            hb[s : s + 1, 128 * h : 128 * h + 128] = rounded[at : at + 1, :]

    hr[y] = hb[...]

    @pl.loop(1, NY, unroll=True)
    def _(k):
        to(hb, hr.at[y], s_h, r_h, {"tp": lax.rem(y + k, NY)})

    for k in (1, 3, 2):
        block = woa.at[:, :, lax.rem(x + NX - k, NX) * NC + c]
        drain(block, r_woa.at[k - 1])
        to(block, block, s_woc, r_woc, partner)

    drain(hr.at[pl.ds(0, NY - 1)], r_h)
    drain(woa.at[:, :, pl.ds(0, NX)], r_woc)
    lined = hr[...].reshape(16, WIDTH).astype(BF)
    attended = jnp.zeros((16, 256), F32)
    for k in range(NY):
        attended = attended + nt(lined[:, 256 * k : 256 * k + 256], woa[k].reshape(256, 256))
    middle = (stream + attended).astype(BF)

    routed = nn(dispatch.astype(BF), middle)
    for k in range(NZ):
        ds[k] = routed[2 * k : 2 * k + 2].astype(ds.dtype)

    @pl.loop(0, NZ, unroll=True)
    def _(k):
        dest, dev = along_z(k)
        to(ds.at[dest], dr.at[k], s_d, r_d.at[lax.div(k, 8)], dev)

    drain(gz_r, r_gz)
    for k in range(NZ):
        gown[2 * k : 2 * k + 2, :] = gz_r[k]
    gall[x] = gown[...]

    @pl.loop(1, NX, unroll=True)
    def _(k):
        to(gown, gall.at[x], s_ga, r_ga, {"ep_1": lax.rem(x + k, NX)})

    @pl.loop(1, NY, unroll=True)
    def _(k):
        to(kvs, kvr.at[y], s_kv, r_kv, {"tp": lax.rem(y + k, NY)})

    rows = NX * 16

    def spread(b):
        drain(dr.at[pl.ds(8 * b, 8)], r_d.at[b])
        for k in range(8):
            lhs[2 * k : 2 * k + 2, :] = dr[8 * b + k].astype(F32)
        xb[b, x, y] = lhs[0:16].astype(BF)

        @pl.loop(0, NX * NY - 1, unroll=True)
        def _(k):
            ox, oy = in_plane(k)
            to(xb.at[b, x, y], xb.at[b, x, y], s_x.at[b], r_x.at[b], {"ep_1": ox, "tp": oy})

    def run_experts(b):
        wide = [xb[b, :, k].reshape(rows, 256).astype(F32) for k in range(NY)]
        total_sq = jnp.zeros((rows, 1), F32)
        for k in range(NY):
            total_sq = total_sq + jnp.sum(wide[k] * wide[k], axis=1, keepdims=True)
        scale = lax.rsqrt(total_sq / WIDTH + norm_eps)
        mixed_in = [(wide[k] * scale * mga[k, 0:1, :]).astype(BF) for k in range(NY)]
        member = gall[:, 16 * b : 16 * b + 16, :].reshape(rows, 128)
        produced = jnp.zeros((rows, WIDTH), F32)
        for e in range(NC):
            gate_act = jnp.zeros((rows, 128), F32)
            up_act = jnp.zeros((rows, 128), F32)
            for k in range(NY):
                gate_act = gate_act + nn(mixed_in[k], gbuf[e, 256 * k : 256 * k + 256, :])
                up_act = up_act + nn(mixed_in[k], ubuf[e, 256 * k : 256 * k + 256, :])
            hidden = (gate_act / (1.0 + jnp.exp(-gate_act)) * up_act).astype(BF)
            slot_gate = jnp.sum(
                jnp.where(iota((rows, 128), 1) == x * NC + e, member, 0.0), axis=1, keepdims=True
            )
            produced = produced + nn(hidden, dbuf[e]) * slot_gate
        for k in range(NX):
            for j in range(NY):
                fs[b, k, j] = produced[16 * k : 16 * k + 16, 256 * j : 256 * j + 256].astype(BF)

        @pl.loop(0, NX * NY - 1, unroll=True)
        def _(k):
            ox, oy = in_plane(k)
            to(fs.at[b, ox, oy], fr.at[b, q16], s_f.at[b], r_f.at[b], {"ep_1": ox, "tp": oy})

        fr[b, q16] = fs[b, x, y]

    def give_back(b):
        drain(fr.at[b, pl.ds(0, NX * NY - 1)], r_f.at[b])
        mixture = fr[b, 0].astype(F32)
        for k in range(1, NX * NY):
            mixture = mixture + fr[b, k].astype(F32)
        for k in range(8):
            zs[8 * b + k] = mixture[2 * k : 2 * k + 2].astype(zs.dtype)

        @pl.loop(8 * b, 8 * b + 8, unroll=True)
        def _(k):
            source = lax.rem(z + 2 * NZ - far_first(k, NZ), NZ)
            to(zs.at[k], zr.at[z], s_z, r_z, {"ep_0": source, "ep_2": 1 - c})

    spread(1)
    spread(0)
    drain(gall.at[pl.ds(0, NX - 1)], r_ga)
    drain(mga.at[pl.ds(0, NY - 1)], r_mg)
    for k, ref in enumerate((gbuf, ubuf, dbuf)):
        drain(ref.at[0], r_ew.at[k])
    drain(fr.at[1, pl.ds(0, NX * NY - 1)], r_x.at[1])
    run_experts(1)
    drain(fr.at[0, pl.ds(0, NX * NY - 1)], r_x.at[0])
    run_experts(0)
    give_back(1)
    give_back(0)

    drain(kvr.at[pl.ds(0, NY - 1)], r_kv)
    for k in range(NY):
        kvo[4 * k : 4 * k + 4, :] = kvr[k, 4:8, :]
    out_ref[1] = kvo[:, 0:256].astype(BF)
    out_ref[2] = kvo[:, 256:512].astype(BF)

    drain(zr, r_z)
    for k in range(NZ):
        lhs[2 * k : 2 * k + 2, :] = zr[k].astype(F32)
    mix = nn(combine.astype(BF), lhs[...].astype(BF))
    out_ref[0] = (middle.astype(F32) + mix).astype(BF)

    for ref, sem in (
        (wzq, s_wzq),
        (wzk, s_wzk),
        (woz.at[0], s_wo),
        (woz.at[pl.ds(0, 3)], s_wo2),
        (gz_r, s_gz),
        (dr, s_d),
        (zr, s_z),
    ):
        drain(ref, sem)
    for ref, sem in ((sqr, s_sq), (mga, s_mg), (kvr, s_kv), (hr, s_h), (woy, s_woy)):
        drain(ref.at[pl.ds(0, NY - 1)], sem)
    drain(nall.at[pl.ds(0, NG - 1)], s_na)
    drain(gall.at[pl.ds(0, NX - 1)], s_ga)
    for k, ref in enumerate((gbuf, ubuf, dbuf)):
        drain(ref.at[0], s_ew.at[k])
    drain(woa.at[:, :, pl.ds(0, NX - 1)], s_woa)
    drain(woa.at[:, :, pl.ds(0, NX)], s_woc)
    drain(rb.at[pl.ds(0, NP - 1)], s_rb)
    for b in range(2):
        drain(fr.at[b, pl.ds(0, NX * NY - 1)], s_x.at[b])
        drain(fr.at[b, pl.ds(0, NX * NY - 1)], s_f.at[b])


def on_device(
    residual,
    cache_keys,
    cache_values,
    lengths,
    query_weight,
    key_weight,
    value_weight,
    out_weight,
    head_gain,
    mix_lambda,
    attn_gain,
    moe_gain,
    route_ids,
    route_logits,
    gate_weight,
    up_weight,
    down_weight,
):
    vm = pl.BlockSpec(memory_space=pltpu.VMEM)
    hbm = pl.BlockSpec(memory_space=pl.ANY)
    dma = pltpu.SemaphoreType.DMA
    V = pltpu.VMEM
    scratch = [
        V((16, 256), BF),
        pltpu.SMEM((16,), jnp.int32),
        V((8, 256), BF),
        V((2, 256), BF),
        V((2, 256), BF),
        V((8, 256), BF),
        V((128,), F32),
        pltpu.SMEM((HEADS,), F32),
        V((256,), BF),
        V((256,), BF),
        V((CHOSEN, 16), jnp.int32),
        V((CHOSEN, 16), F32),
        V((OWN, CACHE, 256), BF),
        V((OWN, CACHE, 256), BF),
        V((NC, WIDTH, 128), BF),
        V((NC, WIDTH, 128), BF),
        V((NC, 128, WIDTH), BF),
        dma((17,)),
        V((4, 256), BF),
        V((NZ, 8, 256), BF),
        V((NZ, 4, 256), BF),
        V((4, NZ // 4, 8, 256), BF),
        V((NY, NZ // NY, 8, 256), BF),
        V((NY, NZ // NY, NG, 8, 256), BF),
        V((16, 128), F32),
        V((NY, 16, 128), F32),
        V((NG, 16, 256), BF),
        V((8, 256), F32),
        V((NY, 8, 256), F32),
        V((NP, 8, 128), F32),
        V((NP, 8, 128), F32),
        V((1024, 768), BF),
        V((NG, 8, 128), F32),
        V((NG, 8, 128), F32),
        V((8, 512), F32),
        V((NY, 8, 512), F32),
        V((16, 512), F32),
        V((OWN, WIDTH), F32),
        V((NY, OWN, WIDTH), F32),
        V((32, 256), F32),
        V((NZ, SLOTS, 128), F32),
        V((NZ, SLOTS, 128), F32),
        V((32, 128), F32),
        V((NX, 32, 128), F32),
        V((NZ, SLOTS, 256), BF),
        V((NZ, SLOTS, 256), BF),
        V((2, NX, NY, 16, 256), BF),
        V((2, NX, NY, 16, 256), BF),
        V((2, NX * NY, 16, 256), BF),
        V((NZ, SLOTS, 256), BF),
        V((NZ, SLOTS, 256), BF),
    ]
    sems = [dma] * 40
    for k in (31, 32, 33, 36, 37):
        sems[k] = dma((2,))
    sems[34] = sems[35] = dma((3,))
    sems[9] = dma((3,))
    results = pl.pallas_call(
        kernel,
        out_shape=pltpu.VMEM((3, 16, 256), BF),
        in_specs=[hbm] * 17,
        out_specs=vm,
        scratch_shapes=scratch + sems,
        compiler_params=pltpu.CompilerParams(collective_id=0, has_side_effects=True),
        cost_estimate=pl.CostEstimate(flops=10**9, bytes_accessed=5 * 10**6, transcendentals=0),
    )(
        residual,
        cache_keys,
        cache_values,
        lengths,
        query_weight.T,
        key_weight.T,
        value_weight.T,
        out_weight.T,
        head_gain,
        mix_lambda,
        attn_gain,
        moe_gain,
        route_ids.T,
        route_logits.T,
        gate_weight,
        up_weight,
        down_weight,
    )
    return results[0], results[1], results[2]


def solution(mesh):
    torus = Mesh(mesh.devices.reshape(NZ, NX, NC, NY), ("ep_0", "ep_1", "ep_2", "tp"))
    return jax.shard_map(
        on_device,
        mesh=torus,
        in_specs=(
            P(EP, "tp"),
            P(EP_TP, None, None),
            P(EP_TP, None, None),
            P(EP),
            P("tp", EP),
            P("tp", EP),
            P("tp", EP),
            P("tp", EP),
            P(),
            P(),
            P("tp"),
            P("tp"),
            P(EP, None),
            P(EP, None),
            P(EP, None, "tp"),
            P(EP, None, "tp"),
            P(EP, "tp", None),
        ),
        out_specs=(P(EP, "tp"), P(EP, None), P(EP, None)),
        check_vma=False,
    )
```

```python
import math

import jax
import jax.numpy as jnp
from jax import lax
from jax.experimental import pallas as pl
from jax.experimental.pallas import tpu as pltpu
from jax.sharding import Mesh
from jax.sharding import PartitionSpec as P

WIDTH = 1024
HEADS = 8
HEAD_DIM = 64
VALUE_DIM = 128
CHOSEN = 6
GROUP_SIZE = 8
SLOTS = 2
EP = ("ep_0", "ep_1", "ep_2")
EP_TP = ("ep_0", "ep_1", "ep_2", "tp")
NZ, NX, NC, NY = 16, 4, 2, 4
NG = NX * NC
NP = NG * NY
CACHE = 1024
OWN = 4

norm_eps = 1e-06
head_eps = 1e-05
masked_score = -1e30
rotary_base = 500000.0

MESH = pl.DeviceIdType.MESH
BF = jnp.bfloat16
F32 = jnp.float32


def nt(a, b):
    return lax.dot_general(a, b, (((1,), (1,)), ((), ())), preferred_element_type=F32)


def nn(a, b):
    return lax.dot_general(a, b, (((1,), (0,)), ((), ())), preferred_element_type=F32)


def far_first(k, n):
    half = lax.div(k + 1, 2)
    return jnp.where(lax.rem(k, 2) == 1, n // 2 + half, n // 2 - half)


def iota(shape, dim):
    return lax.broadcasted_iota(jnp.int32, shape, dim)


def kernel(
    res_hbm,
    ck_hbm,
    cv_hbm,
    lens_hbm,
    wq_hbm,
    wk_hbm,
    wv_hbm,
    wo_hbm,
    hgain_hbm,
    lam_hbm,
    again_hbm,
    mgain_hbm,
    ridt_hbm,
    logitst_hbm,
    gate_hbm,
    up_hbm,
    down_hbm,
    out_ref,
    res_ref,
    lens_ref,
    wq_ref,
    wk_ref,
    wv_ref,
    wo_ref,
    hgain_ref,
    lam_ref,
    again_ref,
    mgain_ref,
    ridt_ref,
    logitst_ref,
    kbuf,
    vbuf,
    gbuf,
    ubuf,
    dbuf,
    loc_sem,
    wkv,
    wzq,
    wzk,
    woz,
    woy,
    woa,
    sqs,
    sqr,
    nall,
    mgs,
    mga,
    sb,
    rb,
    ebuf,
    cosb,
    sinb,
    kvs,
    kvr,
    kvo,
    hb,
    hr,
    lhs,
    gz_s,
    gz_r,
    gown,
    gall,
    ds,
    dr,
    xb,
    fs,
    fr,
    zs,
    zr,
    s_wzq,
    r_wzq,
    s_wzk,
    r_wzk,
    s_wo,
    r_wo,
    s_wo2,
    r_wo2,
    s_woa,
    r_woa,
    s_sq,
    r_sq,
    s_na,
    r_na,
    s_mg,
    r_mg,
    s_rb,
    r_rb,
    s_kv,
    r_kv,
    s_h,
    r_h,
    s_woc,
    r_woc,
    s_woy,
    r_woy,
    s_gz,
    r_gz,
    s_ga,
    r_ga,
    s_d,
    r_d,
    s_x,
    r_x,
    s_ew,
    r_ew,
    s_f,
    r_f,
    s_z,
    r_z,
):
    z = lax.axis_index("ep_0")
    x = lax.axis_index("ep_1")
    c = lax.axis_index("ep_2")
    y = lax.axis_index("tp")
    g = x * NC + c
    p = g * NY + y
    twin = x * NC + 1 - c
    q16 = x * NY + y

    def plane_id(other):
        og = lax.div(other, NY)
        return {"ep_1": lax.div(og, NC), "ep_2": lax.rem(og, NC), "tp": lax.rem(other, NY)}

    def along_z(k):
        dest = lax.rem(z + far_first(k, NZ), NZ)
        return dest, {"ep_0": dest, "ep_2": 1 - c}

    def in_plane(k):
        ox = lax.rem(x + far_first(lax.div(k, NY), NX), NX)
        oy = lax.rem(y + far_first(lax.rem(k, NY), NY), NY)
        return ox, oy

    def to(src, dst, ssem, rsem, dev):
        pltpu.make_async_remote_copy(
            src_ref=src, dst_ref=dst, send_sem=ssem, recv_sem=rsem, device_id=dev, device_id_type=MESH
        ).start()

    def drain(ref, sem):
        pltpu.make_async_copy(ref, ref, sem).wait()

    barrier = pltpu.get_barrier_semaphore()

    @pl.loop(0, NZ - 1, unroll=True)
    def _(k):
        pl.semaphore_signal(barrier, inc=1, device_id=along_z(k)[1], device_id_type=MESH)

    for step in (1, 14, 15):
        pl.semaphore_signal(
            barrier, inc=1, device_id={"ep_0": lax.rem(z + step, NZ)}, device_id_type=MESH
        )

    @pl.loop(1, NP, unroll=True)
    def _(k):
        pl.semaphore_signal(
            barrier, inc=1, device_id=plane_id(lax.rem(p + k, NP)), device_id_type=MESH
        )

    small = [
        pltpu.make_async_copy(src, dst, loc_sem.at[k])
        for k, (src, dst) in enumerate(
            (
                (res_hbm, res_ref),
                (wq_hbm, wq_ref),
                (wk_hbm, wk_ref),
                (wv_hbm, wv_ref),
                (wo_hbm, wo_ref),
                (mgain_hbm, mgain_ref),
                (again_hbm, again_ref),
                (hgain_hbm, hgain_ref),
                (ridt_hbm, ridt_ref),
                (logitst_hbm, logitst_ref),
                (lens_hbm, lens_ref),
                (lam_hbm, lam_ref),
            )
        )
    ]
    experts = [
        pltpu.make_async_copy(gate_hbm.at[0], gbuf.at[c], loc_sem.at[12]),
        pltpu.make_async_copy(up_hbm.at[0], ubuf.at[c], loc_sem.at[13]),
        pltpu.make_async_copy(down_hbm.at[0], dbuf.at[c], loc_sem.at[14]),
    ]
    caches = [
        pltpu.make_async_copy(ck_hbm, kbuf, loc_sem.at[15]),
        pltpu.make_async_copy(cv_hbm, vbuf, loc_sem.at[16]),
    ]
    for copy in small + experts + caches:
        copy.start()
    for copy in small:
        copy.wait()
    wkv[...] = jnp.concatenate([wk_ref[...].astype(F32), wv_ref[...].astype(F32)], axis=0).astype(BF)
    stream = res_ref[...].astype(F32)
    own_squares = jnp.broadcast_to(jnp.sum(stream * stream, axis=1, keepdims=True), (16, 128))
    sqs[...] = own_squares
    mgs[...] = jnp.broadcast_to(mgain_ref[...].astype(F32).reshape(1, 256), (8, 256))

    groups = lax.shift_right_logical(ridt_ref[0:1, :], 3).astype(F32)
    grow = jnp.broadcast_to(groups, (16, 16))
    eye = (iota((16, 16), 0) == iota((16, 16), 1)).astype(F32)
    gcol = nt(eye, grow)
    before = jnp.logical_and(grow == gcol, iota((16, 16), 0) < iota((16, 16), 1))
    rank = jnp.sum(jnp.where(before, 1.0, 0.0), axis=0, keepdims=True)
    slot = groups * SLOTS + rank
    dispatch = jnp.where(iota((32, 16), 0).astype(F32) == slot, 1.0, 0.0)
    combine = nt(eye, dispatch)
    logits = logitst_ref[...]
    exps = jnp.exp(logits - jnp.max(logits, axis=0, keepdims=True))
    gates = exps / jnp.sum(exps, axis=0, keepdims=True)
    members = jnp.zeros((128, 16), F32)
    for k in range(CHOSEN):
        member = jnp.bitwise_and(ridt_ref[k : k + 1, :], GROUP_SIZE - 1)
        members = members + jnp.where(iota((128, 16), 0) == member, gates[k : k + 1, :], 0.0)
    slot_gates = lax.dot_general(
        dispatch, members, (((1,), (1,)), ((), ())), precision=lax.Precision.HIGHEST,
        preferred_element_type=F32,
    )
    for k in range(NZ):
        gz_s[k] = slot_gates[2 * k : 2 * k + 2]

    row = iota((1024, 256), 0)
    col = iota((1024, 256), 1)
    src_g = jnp.bitwise_xor(lax.shift_right_logical(row, 7), 1)
    src_lane = jnp.bitwise_and(row, 127)
    to_query = jnp.bitwise_and(col, 63) == src_g * 8 + jnp.bitwise_and(src_lane, 7)
    ebuf[:, 0:256] = jnp.where(to_query, 1.0, 0.0).astype(BF)
    src_r = jnp.bitwise_and(src_lane, 3)
    spot = lax.shift_right_logical(src_lane, 2) * 16 + src_g * 2 + jnp.bitwise_and(src_r, 1)
    on_spot = jnp.logical_and(col == spot, src_lane < 64)
    ebuf[:, 256:512] = jnp.where(jnp.logical_and(on_spot, src_r < 2), 1.0, 0.0).astype(BF)
    ebuf[:, 512:768] = jnp.where(jnp.logical_and(on_spot, src_r >= 2), 1.0, 0.0).astype(BF)

    lane = iota((8, 128), 1)
    sub = iota((8, 128), 0)
    place = jnp.zeros((8, 128), F32)
    for s in range(OWN):
        place = jnp.where(
            jnp.bitwise_and(sub, 3) == s, lens_ref[y * OWN + s].astype(F32), place
        )
    for k in range(NG):
        at_query = ((k ^ 1) % (NG // 2)) * 8 + jnp.bitwise_and(lane, 7)
        at_key = (
            jnp.bitwise_and(lax.shift_right_logical(lane, 2), 1) * 16
            + (k ^ 1) * 2
            + jnp.bitwise_and(lane, 1)
        )
        entry = jnp.where(sub < 4, at_query, at_key).astype(F32)
        angle = place * jnp.exp(entry * (-math.log(rotary_base) / (HEAD_DIM // 2)))
        cosb[k] = jnp.cos(angle)
        sinb[k] = jnp.sin(angle)

    pl.semaphore_wait(barrier, NZ - 1 + NP - 1 + 3)

    @pl.loop(1, NY, unroll=True)
    def _(k):
        dev = {"tp": lax.rem(y + k, NY)}
        to(sqs, sqr.at[y], s_sq, r_sq, dev)
        to(mgs, mga.at[y], s_mg, r_mg, dev)

    z_low, z_high = lax.rem(z, 4), lax.div(z, 4)
    for step in (8, 4, 12, 0):
        dev = {"ep_0": lax.rem(z + step, NZ), "ep_2": 1 - c}
        to(wo_ref, woz.at[z_low, z_high], s_wo, r_wo, dev)

    @pl.loop(0, NZ, unroll=True)
    def _(k):
        dev = along_z(k)[1]
        to(wq_ref, wzq.at[z], s_wzq, r_wzq, dev)
        to(wkv, wzk.at[z], s_wzk, r_wzk, dev)

    sqr[y] = own_squares
    mga[y] = mgs[...]
    drain(sqr.at[pl.ds(0, NY - 1)], r_sq)
    squares = sqr[0] + sqr[1] + sqr[2] + sqr[3]
    scale = lax.rsqrt(squares[:, 0:1] / WIDTH + norm_eps)
    normed = (stream * scale * again_ref[...].astype(F32).reshape(1, 256)).astype(BF)
    nall[g] = normed

    @pl.loop(1, NG, unroll=True)
    def _(k):
        other = lax.rem(g + k, NG)
        to(
            nall.at[g], nall.at[g], s_na, r_na,
            {"ep_1": lax.div(other, NC), "ep_2": lax.rem(other, NC)},
        )

    @pl.loop(0, NZ, unroll=True)
    def _(k):
        dest, dev = along_z(k)
        to(gz_s.at[dest], gz_r.at[k], s_gz, r_gz, dev)

    partner = {"ep_2": 1 - c}
    for copy in experts:
        copy.wait()
    for k, ref in enumerate((gbuf, ubuf, dbuf)):
        to(ref.at[c], ref.at[c], s_ew.at[k], r_ew.at[k], partner)

    drain(nall.at[pl.ds(0, NG - 1)], r_na)
    drain(woz.at[0], r_wo)
    for step in (2, 1, 15):
        to(woz.at[z_low], woz.at[z_low], s_wo2, r_wo2, {"ep_0": lax.rem(z + step, NZ)})

    drain(wzq, r_wzq)
    drain(wzk, r_wzk)
    tokens = nall[...].reshape(128, 256)
    part_q = nt(tokens, wzq[...].reshape(128, 256))
    part_kv = nt(tokens, wzk[...].reshape(64, 256))
    part_kv = jnp.concatenate([part_kv, jnp.zeros((128, 64), F32)], axis=1)
    for k in range(NP):
        sb[k, 0:4, :] = part_q[4 * k : 4 * k + 4]
        sb[k, 4:8, :] = part_kv[4 * k : 4 * k + 4]

    @pl.loop(0, NX * NY, unroll=True)
    def _(k):
        ox, oy = in_plane(k)
        other = (ox * NC + 1 - c) * NY + oy
        to(sb.at[other], rb.at[p], s_rb, r_rb, plane_id(other))

        @pl.when(k < NX * NY - 1)
        def _():
            same = (ox * NC + c) * NY + oy
            to(sb.at[same], rb.at[p], s_rb, r_rb, plane_id(same))

    rb[p] = sb[p]

    drain(woz.at[pl.ds(0, 3)], r_wo2)
    woy[y] = woz[:, y]
    over_x = [(k, {"ep_1": lax.rem(x + k, NX), "ep_2": 1 - c}) for k in (2, 1, 3)]

    @pl.loop(1, NY, unroll=True)
    def _(k):
        other = lax.rem(y + k, NY)
        to(woz.at[:, other], woy.at[y], s_woy, r_woy, {"tp": other})

    for k, dev in over_x:
        to(woz.at[:, y], woa.at[y, :, twin], s_woa, r_woa.at[k - 1], dev)

    drain(woy.at[pl.ds(0, NY - 1)], r_woy)
    for k, dev in over_x:
        for j in range(1, NY):
            piece = lax.rem(y + j, NY)
            to(woy.at[piece], woa.at[piece, :, twin], s_woa, r_woa.at[k - 1], dev)

    to(woy, woa.at[:, :, twin], s_woc, r_woc, partner)
    woa[:, :, twin] = woy[...]

    drain(rb.at[pl.ds(0, NP - 1)], r_rb)
    parts = rb[...].reshape(NG, NY, 8, 128)
    raw = parts[:, 0] + parts[:, 1] + parts[:, 2] + parts[:, 3]
    is_query = sub < 4
    is_key = jnp.logical_and(lane < 64, jnp.bitwise_and(lane, 3) < 2)
    low_key = jnp.bitwise_and(lane, 15) < 8
    turned = []
    for k in range(NG):
        own = raw[k]
        pair = raw[(k + NG // 2) % NG]
        if k < NG // 2:
            pair = -pair
        above = pltpu.roll(own, 120, 1)
        below = pltpu.roll(own, 8, 1)
        key_pair = jnp.where(low_key, -above, below)
        spun = own * cosb[k] + jnp.where(is_query, pair, key_pair) * sinb[k]
        turned.append(jnp.where(jnp.logical_or(is_query, is_key), spun, own))
    rows8 = jnp.concatenate([t.astype(BF) for t in turned], axis=1)
    placed = nn(rows8, ebuf[:, 256:768])
    kvs[...] = placed
    kvr[y] = placed

    own_keys = placed[4:8, 0:256]
    own_values = placed[4:8, 256:512]

    pieces = []
    for s in range(OWN):
        for m in range(2):
            keep = lax.shift_right_logical(lane, 3) == 2 * sub + m
            line = []
            for k in range(NG):
                whole = jnp.broadcast_to(turned[k][s : s + 1, :], (8, 128))
                line.append(jnp.where(keep, whole, 0.0))
            pieces.append(jnp.concatenate(line, axis=1))
    spread = nn(jnp.concatenate(pieces, axis=0).astype(BF), ebuf[:, 0:256])
    for copy in caches:
        copy.wait()
    blk = lax.shift_right_logical(iota((16, 256), 1), 6)
    row16 = iota((16, 256), 0)
    own_block = (
        lax.shift_right_logical(jnp.bitwise_and(row16, 7), 2) * 2 + lax.shift_right_logical(row16, 3)
    )
    head_low = jnp.bitwise_and(iota((16, 128), 0), 7) < 4
    lam = jnp.zeros((8, 128), F32)
    for h in range(HEADS):
        lam = jnp.where(sub == h, lam_ref[h], lam)
    queries = [jnp.where(blk == own_block, spread[16 * s : 16 * s + 16], 0.0) for s in range(OWN)]
    scores = jnp.concatenate([nt(queries[s].astype(BF), kbuf[s]) for s in range(OWN)], axis=0) * 0.125
    fresh = jnp.concatenate(
        [jnp.sum(queries[s] * own_keys[s : s + 1], axis=1, keepdims=True) for s in range(OWN)], axis=0
    ) * 0.125
    seq_of = lax.shift_right_logical(iota((16 * OWN, 1), 0), 4)
    length = jnp.zeros((16 * OWN, 1), jnp.int32)
    for s in range(OWN):
        length = jnp.where(seq_of == s, lens_ref[y * OWN + s], length)
    scores = jnp.where(iota((16 * OWN, CACHE), 1) < length, scores, masked_score)
    top = jnp.maximum(jnp.max(scores, axis=1, keepdims=True), fresh)
    weights = jnp.exp(scores - top).astype(BF)
    fresh_weight = jnp.exp(fresh - top).astype(BF).astype(F32)
    total = jnp.sum(weights.astype(F32), axis=1, keepdims=True) + fresh_weight
    mixed = [nn(weights[16 * s : 16 * s + 16], vbuf[s]) for s in range(OWN)]
    contrasts = []
    for s in range(OWN):
        here = slice(16 * s, 16 * s + 16)
        fresh_here = fresh_weight[here]
        values = jnp.where(
            head_low,
            mixed[s][:, 0:128] + fresh_here * own_values[s : s + 1, 0:128],
            mixed[s][:, 128:256] + fresh_here * own_values[s : s + 1, 128:256],
        )
        averaged = values / total[here]
        contrasts.append(averaged[0:8] - lam * averaged[8:16])
    contrast = jnp.concatenate(contrasts, axis=0)
    contrast = (
        contrast
        * lax.rsqrt(jnp.mean(contrast * contrast, axis=1, keepdims=True) + head_eps)
        * hgain_ref[...].reshape(1, 128)
    )
    rounded = contrast.astype(BF).astype(F32)
    for s in range(OWN):
        for h in range(HEADS):
            at = HEADS * s + h
            hb[s : s + 1, 128 * h : 128 * h + 128] = rounded[at : at + 1, :]

    hr[y] = hb[...]

    @pl.loop(1, NY, unroll=True)
    def _(k):
        to(hb, hr.at[y], s_h, r_h, {"tp": lax.rem(y + k, NY)})

    for k in (1, 3, 2):
        block = woa.at[:, :, lax.rem(x + NX - k, NX) * NC + c]
        drain(block, r_woa.at[k - 1])
        to(block, block, s_woc, r_woc, partner)

    drain(hr.at[pl.ds(0, NY - 1)], r_h)
    drain(woa.at[:, :, pl.ds(0, NX)], r_woc)
    lined = hr[...].reshape(16, WIDTH).astype(BF)
    attended = jnp.zeros((16, 256), F32)
    for k in range(NY):
        attended = attended + nt(lined[:, 256 * k : 256 * k + 256], woa[k].reshape(256, 256))
    middle = (stream + attended).astype(BF)

    routed = nn(dispatch.astype(BF), middle)
    for k in range(NZ):
        ds[k] = routed[2 * k : 2 * k + 2].astype(ds.dtype)

    @pl.loop(0, NZ, unroll=True)
    def _(k):
        dest, dev = along_z(k)
        to(ds.at[dest], dr.at[k], s_d, r_d.at[lax.div(k, 8)], dev)

    drain(gz_r, r_gz)
    for k in range(NZ):
        gown[2 * k : 2 * k + 2, :] = gz_r[k]
    gall[x] = gown[...]

    @pl.loop(1, NX, unroll=True)
    def _(k):
        to(gown, gall.at[x], s_ga, r_ga, {"ep_1": lax.rem(x + k, NX)})

    @pl.loop(1, NY, unroll=True)
    def _(k):
        to(kvs, kvr.at[y], s_kv, r_kv, {"tp": lax.rem(y + k, NY)})

    rows = NX * 16

    def spread(b):
        drain(dr.at[pl.ds(8 * b, 8)], r_d.at[b])
        for k in range(8):
            lhs[2 * k : 2 * k + 2, :] = dr[8 * b + k].astype(F32)
        xb[b, x, y] = lhs[0:16].astype(BF)

        @pl.loop(0, NX * NY - 1, unroll=True)
        def _(k):
            ox, oy = in_plane(k)
            to(xb.at[b, x, y], xb.at[b, x, y], s_x.at[b], r_x.at[b], {"ep_1": ox, "tp": oy})

    def run_experts(b):
        wide = [xb[b, :, k].reshape(rows, 256).astype(F32) for k in range(NY)]
        total_sq = jnp.zeros((rows, 1), F32)
        for k in range(NY):
            total_sq = total_sq + jnp.sum(wide[k] * wide[k], axis=1, keepdims=True)
        scale = lax.rsqrt(total_sq / WIDTH + norm_eps)
        mixed_in = [(wide[k] * scale * mga[k, 0:1, :]).astype(BF) for k in range(NY)]
        member = gall[:, 16 * b : 16 * b + 16, :].reshape(rows, 128)
        produced = jnp.zeros((rows, WIDTH), F32)
        for e in range(NC):
            gate_act = jnp.zeros((rows, 128), F32)
            up_act = jnp.zeros((rows, 128), F32)
            for k in range(NY):
                gate_act = gate_act + nn(mixed_in[k], gbuf[e, 256 * k : 256 * k + 256, :])
                up_act = up_act + nn(mixed_in[k], ubuf[e, 256 * k : 256 * k + 256, :])
            hidden = (gate_act / (1.0 + jnp.exp(-gate_act)) * up_act).astype(BF)
            slot_gate = jnp.sum(
                jnp.where(iota((rows, 128), 1) == x * NC + e, member, 0.0), axis=1, keepdims=True
            )
            produced = produced + nn(hidden, dbuf[e]) * slot_gate
        for k in range(NX):
            for j in range(NY):
                fs[b, k, j] = produced[16 * k : 16 * k + 16, 256 * j : 256 * j + 256].astype(BF)

        @pl.loop(0, NX * NY - 1, unroll=True)
        def _(k):
            ox, oy = in_plane(k)
            to(fs.at[b, ox, oy], fr.at[b, q16], s_f.at[b], r_f.at[b], {"ep_1": ox, "tp": oy})

        fr[b, q16] = fs[b, x, y]

    def give_back(b):
        drain(fr.at[b, pl.ds(0, NX * NY - 1)], r_f.at[b])
        mixture = fr[b, 0].astype(F32)
        for k in range(1, NX * NY):
            mixture = mixture + fr[b, k].astype(F32)
        for k in range(8):
            zs[8 * b + k] = mixture[2 * k : 2 * k + 2].astype(zs.dtype)

        @pl.loop(8 * b, 8 * b + 8, unroll=True)
        def _(k):
            source = lax.rem(z + 2 * NZ - far_first(k, NZ), NZ)
            to(zs.at[k], zr.at[z], s_z, r_z, {"ep_0": source, "ep_2": 1 - c})

    spread(1)
    spread(0)
    drain(gall.at[pl.ds(0, NX - 1)], r_ga)
    drain(mga.at[pl.ds(0, NY - 1)], r_mg)
    for k, ref in enumerate((gbuf, ubuf, dbuf)):
        drain(ref.at[0], r_ew.at[k])
    drain(fr.at[1, pl.ds(0, NX * NY - 1)], r_x.at[1])
    run_experts(1)
    drain(fr.at[0, pl.ds(0, NX * NY - 1)], r_x.at[0])
    run_experts(0)
    give_back(1)
    give_back(0)

    drain(kvr.at[pl.ds(0, NY - 1)], r_kv)
    for k in range(NY):
        kvo[4 * k : 4 * k + 4, :] = kvr[k, 4:8, :]
    out_ref[1] = kvo[:, 0:256].astype(BF)
    out_ref[2] = kvo[:, 256:512].astype(BF)

    drain(zr, r_z)
    for k in range(NZ):
        lhs[2 * k : 2 * k + 2, :] = zr[k].astype(F32)
    mix = nn(combine.astype(BF), lhs[...].astype(BF))
    out_ref[0] = (middle.astype(F32) + mix).astype(BF)

    for ref, sem in (
        (wzq, s_wzq),
        (wzk, s_wzk),
        (woz.at[0], s_wo),
        (woz.at[pl.ds(0, 3)], s_wo2),
        (gz_r, s_gz),
        (dr, s_d),
        (zr, s_z),
    ):
        drain(ref, sem)
    for ref, sem in ((sqr, s_sq), (mga, s_mg), (kvr, s_kv), (hr, s_h), (woy, s_woy)):
        drain(ref.at[pl.ds(0, NY - 1)], sem)
    drain(nall.at[pl.ds(0, NG - 1)], s_na)
    drain(gall.at[pl.ds(0, NX - 1)], s_ga)
    for k, ref in enumerate((gbuf, ubuf, dbuf)):
        drain(ref.at[0], s_ew.at[k])
    drain(woa.at[:, :, pl.ds(0, NX - 1)], s_woa)
    drain(woa.at[:, :, pl.ds(0, NX)], s_woc)
    drain(rb.at[pl.ds(0, NP - 1)], s_rb)
    for b in range(2):
        drain(fr.at[b, pl.ds(0, NX * NY - 1)], s_x.at[b])
        drain(fr.at[b, pl.ds(0, NX * NY - 1)], s_f.at[b])


def on_device(
    residual,
    cache_keys,
    cache_values,
    lengths,
    query_weight,
    key_weight,
    value_weight,
    out_weight,
    head_gain,
    mix_lambda,
    attn_gain,
    moe_gain,
    route_ids,
    route_logits,
    gate_weight,
    up_weight,
    down_weight,
):
    vm = pl.BlockSpec(memory_space=pltpu.VMEM)
    hbm = pl.BlockSpec(memory_space=pl.ANY)
    dma = pltpu.SemaphoreType.DMA
    V = pltpu.VMEM
    scratch = [
        V((16, 256), BF),
        pltpu.SMEM((16,), jnp.int32),
        V((8, 256), BF),
        V((2, 256), BF),
        V((2, 256), BF),
        V((8, 256), BF),
        V((128,), F32),
        pltpu.SMEM((HEADS,), F32),
        V((256,), BF),
        V((256,), BF),
        V((CHOSEN, 16), jnp.int32),
        V((CHOSEN, 16), F32),
        V((OWN, CACHE, 256), BF),
        V((OWN, CACHE, 256), BF),
        V((NC, WIDTH, 128), BF),
        V((NC, WIDTH, 128), BF),
        V((NC, 128, WIDTH), BF),
        dma((17,)),
        V((4, 256), BF),
        V((NZ, 8, 256), BF),
        V((NZ, 4, 256), BF),
        V((4, NZ // 4, 8, 256), BF),
        V((NY, NZ // NY, 8, 256), BF),
        V((NY, NZ // NY, NG, 8, 256), BF),
        V((16, 128), F32),
        V((NY, 16, 128), F32),
        V((NG, 16, 256), BF),
        V((8, 256), F32),
        V((NY, 8, 256), F32),
        V((NP, 8, 128), F32),
        V((NP, 8, 128), F32),
        V((1024, 768), BF),
        V((NG, 8, 128), F32),
        V((NG, 8, 128), F32),
        V((8, 512), F32),
        V((NY, 8, 512), F32),
        V((16, 512), F32),
        V((OWN, WIDTH), F32),
        V((NY, OWN, WIDTH), F32),
        V((32, 256), F32),
        V((NZ, SLOTS, 128), F32),
        V((NZ, SLOTS, 128), F32),
        V((32, 128), F32),
        V((NX, 32, 128), F32),
        V((NZ, SLOTS, 256), BF),
        V((NZ, SLOTS, 256), BF),
        V((2, NX, NY, 16, 256), BF),
        V((2, NX, NY, 16, 256), BF),
        V((2, NX * NY, 16, 256), BF),
        V((NZ, SLOTS, 256), BF),
        V((NZ, SLOTS, 256), BF),
    ]
    sems = [dma] * 40
    for k in (31, 32, 33, 36, 37):
        sems[k] = dma((2,))
    sems[34] = sems[35] = dma((3,))
    sems[9] = dma((3,))
    results = pl.pallas_call(
        kernel,
        out_shape=pltpu.VMEM((3, 16, 256), BF),
        in_specs=[hbm] * 17,
        out_specs=vm,
        scratch_shapes=scratch + sems,
        compiler_params=pltpu.CompilerParams(collective_id=0, has_side_effects=True),
        cost_estimate=pl.CostEstimate(flops=10**9, bytes_accessed=5 * 10**6, transcendentals=0),
    )(
        residual,
        cache_keys,
        cache_values,
        lengths,
        query_weight.T,
        key_weight.T,
        value_weight.T,
        out_weight.T,
        head_gain,
        mix_lambda,
        attn_gain,
        moe_gain,
        route_ids.T,
        route_logits.T,
        gate_weight,
        up_weight,
        down_weight,
    )
    return results[0], results[1], results[2]


def solution(mesh):
    torus = Mesh(mesh.devices.reshape(NZ, NX, NC, NY), ("ep_0", "ep_1", "ep_2", "tp"))
    return jax.shard_map(
        on_device,
        mesh=torus,
        in_specs=(
            P(EP, "tp"),
            P(EP_TP, None, None),
            P(EP_TP, None, None),
            P(EP),
            P("tp", EP),
            P("tp", EP),
            P("tp", EP),
            P("tp", EP),
            P(),
            P(),
            P("tp"),
            P("tp"),
            P(EP, None),
            P(EP, None),
            P(EP, None, "tp"),
            P(EP, None, "tp"),
            P(EP, "tp", None),
        ),
        out_specs=(P(EP, "tp"), P(EP, None), P(EP, None)),
        check_vma=False,
    )
```
